512 devices in a mesh: ep: 32 (over z, x), tp: 16 (over y, core).
Axes of the slice: x: 4, y: 8, z: 8, core: 2. Of those that a mesh axis runs over, the one named last changes fastest.
Arguments:
- queries: bfloat16 [196608, 1024], P(('ep', 'tp')), may hold values from -250 to 250
- keys_values: bfloat16 [2, 196608, 256], P(None, ('ep', 'tp')), may hold values from -8 to 8
- sink_logits: float32 [16], replicated, may hold values from 2 to 6
- moe_rows: bfloat16 [8192, 2048], P('ep'), may hold values from -600 to 600
- norm_gain: float32 [2048], replicated, may hold values from 0.1 to 1.9
- group_choice: int32 [8192], P('ep'), may hold values from 0 to 7, as said below
- member_choice: int32 [8192, 2], P('ep'), may hold values from 0 to 3, as said below
- route_weight: float32 [8192, 2], P('ep'), may hold values from 0.1 to 1
- w_gate: bfloat16 [32, 2048, 2048], P('ep', None, 'tp'), may hold values from -0.125 to 0.125
- w_up: bfloat16 [32, 2048, 2048], P('ep', None, 'tp'), may hold values from -0.125 to 0.125
- w_down: bfloat16 [32, 2048, 2048], P('ep', None, 'tp'), may hold values from -0.125 to 0.125
Outputs:
- attended: bfloat16 [196608, 1024], P(('ep', 'tp'))
- mixed: bfloat16 [8192, 2048], P('ep', 'tp')
The draws below stay inside these ranges and needn't reach their ends.
Inputs may be any that keep to these rules, and one draw needn't show every extreme that they name: With expert = group_choice * 4 + member_choice, within the 256 rows of one index of ep no expert is named by more than 32 rows, and some expert is named by exactly 32 rows. `member_choice`: the 2 entries of a row differ.
All inputs are finite; a program needn't handle non-finite values.
Results may differ from the reference program's by a relative error of at most 0.007.
Values may be sent and summed in bfloat16 or wider, within the bound.
No kernel may reach another device: no remote copies, remote signals or barrier semaphores. Data moves between devices by JAX's collectives and lax.ppermute only.
A program may use at most 64 MiB of HBM per device.

```python
import math
import jax
import jax.numpy as jnp
from jax import lax

D = 2048
QH = 16
KVH = 4
HD = 64
WINDOW = 128
MOE_ROWS = 256
FF = 2048
EPG = 4
TOP = 2
EXPERTS = 32
ATOKENS = 196608
MOE_TOKENS = 8192
CAP = 32
N_EP = 32


def attention_pair(key):
    base_key = jax.random.fold_in(key, 101)
    seed_query, seed_keys, seed_value = jax.random.split(base_key, 3)
    queries = 1.5 * jax.random.normal(seed_query, (ATOKENS, QH * HD), jnp.float32)
    key_rows = jax.random.normal(seed_keys, (ATOKENS, KVH, HD), jnp.float32)
    values = 2.0 * jax.random.normal(seed_value, (ATOKENS, KVH * HD), jnp.float32)
    queries = jnp.clip(queries, -250.0, 250.0)
    stacked = jnp.clip(jnp.stack([key_rows.reshape(ATOKENS, KVH * HD), values]), -8.0, 8.0)
    return (queries.astype(jnp.bfloat16), stacked.astype(jnp.bfloat16))


def draw_queries(key, part):
    return attention_pair(key)[0]


def draw_keys_values(key, part):
    return attention_pair(key)[1]


def draw_moe_rows(key, part):
    base_key = jax.random.fold_in(key, 202)
    seed_rows, seed_columns, seed_noise = jax.random.split(base_key, 3)
    row_scale = jnp.exp(jax.random.uniform(seed_rows, (MOE_TOKENS, 1), jnp.float32, 0.0, math.log(10.0)))
    column_scale = jnp.exp(jax.random.uniform(seed_columns, (1, D), jnp.float32, 0.0, math.log(10.0)))
    values = row_scale * column_scale * jax.random.normal(seed_noise, (MOE_TOKENS, D), jnp.float32)
    return jnp.clip(values, -600.0, 600.0).astype(jnp.bfloat16)


def route_pair(key):
    base_key = jax.random.fold_in(key, 303)
    groups = EXPERTS // EPG
    seat_count = CAP * EPG // TOP
    star_rows = (CAP - 1) * EPG // TOP + 1
    others = MOE_ROWS - star_rows
    blocks = MOE_TOKENS // MOE_ROWS
    seed_star, seed_order, seed_blocks = jax.random.split(base_key, 3)
    star_group = jax.random.randint(seed_star, (), 0, groups)
    star_order = jax.random.permutation(seed_order, EPG)

    def one_block(block_key):
        seed_seat, seed_perm, seed_shuffle = jax.random.split(block_key, 3)
        seat_order = jax.random.permutation(seed_seat, (groups - 1) * seat_count)[:others]
        other_group = seat_order // seat_count
        other_group = other_group + (other_group >= star_group).astype(jnp.int32)
        group_all = jnp.concatenate([jnp.full((star_rows,), star_group, jnp.int32), other_group.astype(jnp.int32)])
        slot_all = jnp.concatenate([jnp.arange(star_rows, dtype=jnp.int32), (seat_order % seat_count).astype(jnp.int32)])
        orders = jax.vmap(lambda seed_one: jax.random.permutation(seed_one, EPG))(jax.random.split(seed_perm, groups))
        orders = jnp.where((jnp.arange(groups) == star_group)[:, None], star_order[None, :], orders)
        columns = (TOP * slot_all[:, None] + jnp.arange(TOP, dtype=jnp.int32)[None, :]) % EPG
        members = orders[group_all[:, None], columns]
        shuffle = jax.random.permutation(seed_shuffle, MOE_ROWS)
        return (group_all[shuffle], members[shuffle])
    group_out, member_out = jax.vmap(one_block)(jax.random.split(seed_blocks, blocks))
    return (group_out.reshape(MOE_TOKENS).astype(jnp.int32), member_out.reshape(MOE_TOKENS, TOP).astype(jnp.int32))


def draw_group_choice(key, part):
    return route_pair(key)[0]


def draw_member_choice(key, part):
    return route_pair(key)[1]


def level_of(key, extent, pieces, least, high):
    loudness = 1.0
    for dim, shards_of in pieces:
        steps = jax.random.uniform(jax.random.fold_in(jax.random.fold_in(key, 6), dim), (shards_of,), jnp.float32, least / len(pieces), high / len(pieces))
        loudness = loudness * jnp.repeat(jnp.exp(steps), extent[dim] // shards_of).reshape((-1,) + (1,) * (len(extent) - 1 - dim))
    return loudness


def bell_draw(key, dims, scale, limit, cuts=(), kind=jnp.bfloat16):
    values = jax.random.normal(key, dims, jnp.float32) * scale
    if len(cuts) > 0:
        values = level_of(key, dims, cuts, -0.22, 0.18) * values
    return jnp.clip(values, min=-limit, max=limit).astype(kind)


def setup_inputs(seed: int = 0) -> dict:
    keys = jax.random.split(jax.random.key(seed), 12)
    queries = draw_queries(jax.random.fold_in(keys[11], 71), 0)
    keys_values = draw_keys_values(jax.random.fold_in(keys[11], 71), 0)
    sink_logits = jnp.clip(jax.random.uniform(keys[2], (QH,), jnp.float32, 2.0, 6.0), 2.0, 6.0)
    moe_rows = draw_moe_rows(jax.random.fold_in(keys[11], 71), 0)
    norm_gain = jnp.clip(1.0 + 0.18 * jax.random.normal(keys[4], (D,), jnp.float32), 0.1, 1.9)
    group_choice = draw_group_choice(jax.random.fold_in(keys[11], 71), 0)
    member_choice = draw_member_choice(jax.random.fold_in(keys[11], 71), 0)
    route_weight = jnp.clip(0.1 + 0.9 * jax.random.uniform(keys[7], (MOE_TOKENS, TOP), jnp.float32) ** level_of(keys[7], (MOE_TOKENS, TOP), ((0, 32),), -0.2, 0.2), 0.1, 1.0)
    w_gate = bell_draw(keys[8], (EXPERTS, D, FF), D ** -0.5, 0.125, ((0, 32), (2, 16)))
    w_up = bell_draw(keys[9], (EXPERTS, D, FF), D ** -0.5, 0.125, ((0, 32), (2, 16)))
    w_down = bell_draw(keys[10], (EXPERTS, FF, D), FF ** -0.5, 0.125, ((0, 32), (2, 16)))
    return {"queries": queries, "keys_values": keys_values, "sink_logits": sink_logits, "moe_rows": moe_rows, "norm_gain": norm_gain, "group_choice": group_choice, "member_choice": member_choice, "route_weight": route_weight, "w_gate": w_gate, "w_up": w_up, "w_down": w_down}


def attend_all(queries, keys_values, sink_logits):
    sharing = QH // KVH
    blocks = ATOKENS // WINDOW
    padded = jnp.pad(keys_values, ((0, 0), (WINDOW, 0), (0, 0)))
    first_half = padded[:, :ATOKENS].reshape(2, blocks, WINDOW, KVH, HD)
    second_half = padded[:, WINDOW:].reshape(2, blocks, WINDOW, KVH, HD)
    banded = jnp.concatenate([first_half, second_half], axis=2)
    query_blocks = queries.reshape(blocks, WINDOW, KVH, sharing, HD)
    key_column = jnp.arange(2 * WINDOW, dtype=jnp.int32)
    distance = jnp.arange(WINDOW, dtype=jnp.int32)[:, None] + WINDOW - key_column[None, :]
    inside = (distance >= 0) & (distance < WINDOW)
    sink_column = sink_logits.reshape(KVH, sharing)[:, :, None]

    def one_block(operands):
        query_block, key_block, value_block, number = operands
        scores = jnp.einsum('qhgd,khd->hgqk', query_block.astype(jnp.float32), key_block.astype(jnp.float32)) * HD ** (-0.5)
        visible = inside & (number * WINDOW + key_column[None, :] - WINDOW >= 0)
        scores = jnp.where(visible[None, None], scores, -1e+30)
        highest = jnp.maximum(lax.optimization_barrier(jnp.max(scores, axis=-1)), sink_column)
        weights = jnp.exp(scores - highest[..., None])
        totals = lax.optimization_barrier(jnp.sum(weights, axis=-1)) + jnp.exp(sink_column - highest)
        rounded = lax.optimization_barrier(weights.astype(jnp.bfloat16)).astype(jnp.float32)
        summed = jnp.einsum('hgqk,khd->qhgd', rounded, value_block.astype(jnp.float32))
        return (summed / jnp.transpose(totals, (2, 0, 1))[..., None]).astype(jnp.bfloat16)
    result = lax.map(one_block, (query_blocks, banded[0], banded[1], jnp.arange(blocks, dtype=jnp.int32)))
    return result.reshape(ATOKENS, QH * HD)

def experts_all(moe_rows, norm_gain, group_choice, member_choice, route_weight, w_gate, w_up, w_down):
    values = moe_rows.astype(jnp.float32)
    normed = (values * lax.rsqrt(lax.optimization_barrier(jnp.mean(values * values, axis=1, keepdims=True)) + 1e-06) * norm_gain).astype(jnp.bfloat16)
    chosen = (group_choice[:, None] * EPG + member_choice).astype(jnp.int32).reshape(N_EP, MOE_ROWS * TOP)
    onehot = (chosen[:, :, None] == jnp.arange(EXPERTS, dtype=jnp.int32)[None, None, :]).astype(jnp.int32)
    earlier = (jnp.cumsum(onehot, axis=1) - onehot).astype(jnp.int32)
    position = lax.optimization_barrier(jnp.sum(earlier * onehot, axis=2)).astype(jnp.int32)
    source = jnp.arange(N_EP, dtype=jnp.int32)[:, None]
    placed = (chosen * (N_EP * CAP) + source * CAP + position).astype(jnp.int32).reshape(MOE_TOKENS, TOP)
    source_row = jnp.arange(MOE_TOKENS * TOP, dtype=jnp.int32) // TOP
    lookup = jnp.full((EXPERTS * N_EP * CAP,), MOE_TOKENS, jnp.int32).at[placed.reshape(-1)].set(source_row)
    padded = jnp.concatenate([normed, jnp.zeros((1, D), jnp.bfloat16)], axis=0)

    def one_expert(operands):
        row_index, gate_weight, up_weight, down_weight = operands
        inputs = padded[row_index]
        gate_part = jnp.dot(inputs, gate_weight, preferred_element_type=jnp.float32)
        up_part = jnp.dot(inputs, up_weight, preferred_element_type=jnp.float32)
        hidden = (jax.nn.silu(gate_part) * up_part).astype(jnp.bfloat16)
        return jnp.dot(hidden, down_weight, preferred_element_type=jnp.float32).astype(jnp.bfloat16)
    produced = lax.map(one_expert, (lookup.reshape(EXPERTS, N_EP * CAP), w_gate, w_up, w_down))
    picked = produced.reshape(EXPERTS * N_EP * CAP, D)[placed].astype(jnp.float32)
    return lax.optimization_barrier(jnp.sum(route_weight[:, :, None] * picked, axis=1)).astype(jnp.bfloat16)

def reference(queries, keys_values, sink_logits, moe_rows, norm_gain, group_choice, member_choice, route_weight, w_gate, w_up, w_down):
    attended = attend_all(queries, keys_values, sink_logits)
    mixed = experts_all(moe_rows, norm_gain, group_choice, member_choice, route_weight, w_gate, w_up, w_down)
    return (attended, mixed)
```

```python
import jax
import jax.numpy as jnp
from jax import lax
from jax.experimental import pallas as pl
from jax.experimental.pallas import tpu as pltpu
from jax.sharding import PartitionSpec as P

QH = 16
KVH = 4
HD = 64
WINDOW = 128
EPG = 4
TOP = 2
LANES = 128
ROW_SCALE = 256.0
EXP_LOW = -60
EXP_COUNT = 80


def attention_kernel(first_ref, sink_ref, q_ref, prev_ref, cur_ref, edge_ref, out_ref):
    block = pl.program_id(0)
    f32 = jnp.float32
    bf16 = jnp.bfloat16
    row = lax.broadcasted_iota(jnp.int32, (WINDOW, WINDOW), 0)
    col = lax.broadcasted_iota(jnp.int32, (WINDOW, WINDOW), 1)
    causal = col <= row
    lane = lax.broadcasted_iota(jnp.int32, (WINDOW, LANES), 1)
    low = lane < HD
    at_start = block == 0
    hidden_prev = jnp.where(at_start, first_ref[0], 0)
    floor = jnp.where(hidden_prev == 1, f32(-1e30), f32(0.0))
    keep = jnp.where(hidden_prev == 1, f32(0.0), f32(1.0))
    zero = jnp.zeros((WINDOW, LANES), bf16)
    for c in range(KVH):
        lanes = pl.ds((c // 2) * LANES, LANES)
        mine = low if c % 2 == 0 else jnp.logical_not(low)
        parts = []
        for which in range(2):
            before = jnp.where(at_start, edge_ref[which, :, lanes], prev_ref[which, :, lanes])
            now = cur_ref[which, :, lanes]
            halves = []
            for value in (before, now):
                own = jnp.where(mine, value, zero)
                swapped = pltpu.roll(own.astype(f32), HD, 1).astype(bf16)
                halves.append((own, swapped) if c % 2 == 0 else (swapped, own))
            (a_prev, b_prev), (a_cur, b_cur) = halves
            parts.append(jnp.concatenate([a_prev, a_cur, b_prev, b_cur], axis=0))
        keys, values = parts
        keys = keys * bf16(HD ** (-0.5))
        for p in range(2):
            head = c * 4 + p * 2
            at = c * 256 + p * LANES
            q = q_ref[:, at : at + LANES]
            scores = lax.dot_general(q, keys, (((1,), (1,)), ((), ())), preferred_element_type=f32)
            pieces = []
            sums = []
            for side in range(2):
                base = side * 2 * WINDOW
                s_prev = scores[:, base : base + WINDOW] * keep + floor
                s_cur = scores[:, base + WINDOW : base + 2 * WINDOW]
                s = jnp.where(causal, s_cur, s_prev)
                sink = sink_ref[head + side]
                highest = jnp.maximum(jnp.max(s, axis=1, keepdims=True), sink)
                w = jnp.exp(s - highest)
                sums.append(jnp.sum(w, axis=1, keepdims=True) + jnp.exp(sink - highest))
                rounded = w.astype(bf16)
                pieces.append(jnp.where(causal, zero, rounded))
                pieces.append(jnp.where(causal, rounded, zero))
            weights = jnp.concatenate(pieces, axis=1)
            summed = jnp.dot(weights, values, preferred_element_type=f32)
            total = jnp.where(low, sums[0], sums[1])
            out_ref[:, at : at + LANES] = (summed / total).astype(bf16)


def attend_window(queries, keys_values, sink_logits):
    length = queries.shape[0]
    blocks = length // WINDOW
    width = keys_values.shape[2]
    edge_rows = keys_values[:, length - WINDOW :, :]
    peers = lax.axis_size(("ep", "tp"))
    pairs = [(i, i + 1) for i in range(peers - 1)]
    edge = lax.ppermute(edge_rows, ("ep", "tp"), pairs)
    first = (lax.axis_index(("ep", "tp")) == 0).astype(jnp.int32).reshape(1)
    return pl.pallas_call(
        attention_kernel,
        grid=(blocks,),
        in_specs=[
            pl.BlockSpec(memory_space=pltpu.SMEM),
            pl.BlockSpec(memory_space=pltpu.SMEM),
            pl.BlockSpec((WINDOW, queries.shape[1]), lambda b: (b, 0)),
            pl.BlockSpec((2, WINDOW, width), lambda b: (0, jnp.maximum(b - 1, 0), 0)),
            pl.BlockSpec((2, WINDOW, width), lambda b: (0, b, 0)),
            pl.BlockSpec((2, WINDOW, width), lambda b: (0, 0, 0)),
        ],
        out_specs=pl.BlockSpec((WINDOW, queries.shape[1]), lambda b: (b, 0)),
        out_shape=jax.ShapeDtypeStruct(queries.shape, jnp.bfloat16),
        cost_estimate=pl.CostEstimate(flops=3 * 10**9, bytes_accessed=3 * 10**6, transcendentals=10**6),
        name="attention",
    )(first, sink_logits, queries, keys_values, keys_values, edge)


def dispatch_kernel(mine_ref, chosen_ref, rows_ref, gain_ref, out_ref, place_ref, normed_ref):
    f32 = jnp.float32
    bf16 = jnp.bfloat16
    tokens = rows_ref.shape[0]
    experts = 32
    capacity = 32
    values = rows_ref[...].astype(f32)
    mean = jnp.mean(values * values, axis=1, keepdims=True)
    normed = (values * lax.rsqrt(mean + 1e-06) * gain_ref[...]).astype(bf16)
    normed_ref[...] = normed * bf16(ROW_SCALE)
    which = lax.broadcasted_iota(jnp.int32, (experts, tokens), 0)
    first = (which == chosen_ref[0:1, :]).astype(f32)
    second = (which == chosen_ref[1:2, :]).astype(f32)
    before = (
        lax.broadcasted_iota(jnp.int32, (tokens, tokens), 0)
        < lax.broadcasted_iota(jnp.int32, (tokens, tokens), 1)
    ).astype(f32).astype(bf16)
    earlier = jnp.dot((first + second).astype(bf16), before, preferred_element_type=f32)
    places = []
    for k, hot in enumerate((first, second)):
        place = jnp.sum(hot * earlier, axis=0, keepdims=True).astype(jnp.int32)
        places.append(chosen_ref[k : k + 1, :] * capacity + place)
    slots = out_ref.shape[0]
    share = slots // experts
    slot = lax.broadcasted_iota(jnp.int32, (slots, tokens), 0)
    wanted = (slot // share) * capacity + mine_ref[0] * share + slot % share
    pick = ((places[0] == wanted) | (places[1] == wanted)).astype(f32).astype(bf16)
    out_ref[...] = jnp.dot(pick, normed_ref[...], preferred_element_type=f32).astype(bf16)
    for k in range(TOP):
        wide = jnp.broadcast_to(places[k].astype(f32), (LANES, tokens))
        place_ref[k] = wide.T.astype(jnp.int32)


def hidden_kernel(x_ref, gate_ref, up_ref, out_ref, hidden_ref):
    f32 = jnp.float32
    bf16 = jnp.bfloat16
    rows = x_ref.shape[0]
    step = 256
    back = f32(1.0 / ROW_SCALE)
    peak = jnp.zeros((8, LANES), f32)
    for i in range(rows // step):
        x = x_ref[i * step : (i + 1) * step, :]
        gate = jnp.dot(x, gate_ref[...], preferred_element_type=f32) * back
        up = jnp.dot(x, up_ref[...], preferred_element_type=f32) * back
        hidden = (gate / (1.0 + jnp.exp(-gate)) * up).astype(bf16)
        hidden_ref[i * step : (i + 1) * step, :] = hidden
        size = jnp.abs(hidden.astype(f32)).reshape(step // 8, 8, LANES)
        peak = jnp.maximum(peak, jnp.max(size, axis=0))
    top = jnp.max(jnp.max(peak, axis=1, keepdims=True), axis=0, keepdims=True)
    index = jnp.zeros((1, 1), f32)
    scale = jnp.full((1, 1), 2.0 ** (14 - EXP_LOW), f32)
    for i in range(1, EXP_COUNT):
        reached = top >= f32(2.0 ** (EXP_LOW + i))
        index = jnp.where(reached, f32(i), index)
        scale = jnp.where(reached, f32(2.0 ** (14 - EXP_LOW - i)), scale)
    for i in range(rows // step):
        part = hidden_ref[i * step : (i + 1) * step, :].astype(f32) * scale
        out_ref[i * step : (i + 1) * step, :] = part.astype(bf16)
    out_ref[rows:, :] = jnp.broadcast_to(index, (16, LANES)).astype(bf16)


def down_kernel(h_ref, w_ref, out_ref):
    f32 = jnp.float32
    bf16 = jnp.bfloat16
    blocks, extended, width = h_ref.shape
    rows = extended - 16
    weights = []
    for t in range(blocks):
        index = h_ref[t, rows : rows + 16, :].astype(f32)[0:1, :]
        scale = jnp.full((1, LANES), 2.0 ** (EXP_LOW - 14), f32)
        for i in range(1, EXP_COUNT):
            scale = jnp.where(index == f32(i), f32(2.0 ** (EXP_LOW - 14 + i)), scale)
        weights.append((w_ref[t * width : (t + 1) * width, :].astype(f32) * scale).astype(bf16))
    step = 256
    for i in range(rows // step):
        acc = jnp.zeros((step, w_ref.shape[1]), f32)
        for t in range(0, blocks, 2):
            left = h_ref[t, i * step : (i + 1) * step, :]
            right = h_ref[t + 1, i * step : (i + 1) * step, :]
            pair = jnp.concatenate([left, right], axis=1)
            weight = jnp.concatenate([weights[t], weights[t + 1]], axis=0)
            acc = acc + jnp.dot(pair, weight, preferred_element_type=f32)
        out_ref[i * step : (i + 1) * step, :] = acc.astype(bf16)


def combine_kernel(place_ref, weight_ref, rows_ref, out_ref):
    f32 = jnp.float32
    bf16 = jnp.bfloat16
    slots = rows_ref.shape[0]
    tokens = out_ref.shape[0]
    total = None
    for k in range(TOP):
        place = place_ref[k]
        hots = []
        for j in range(slots // LANES):
            slot = lax.broadcasted_iota(jnp.int32, (tokens, LANES), 1) + j * LANES
            hots.append((place == slot).astype(f32).astype(bf16))
        hot = jnp.concatenate(hots, axis=1)
        picked = jnp.dot(hot, rows_ref[...], preferred_element_type=f32)
        part = weight_ref[:, k : k + 1] * picked
        total = part if total is None else total + part
    out_ref[...] = total.astype(bf16)


def route_experts(
    moe_rows, norm_gain, group_choice, member_choice, route_weight, w_gate, w_up, w_down
):
    bf16 = jnp.bfloat16
    tokens, width = moe_rows.shape
    experts = 32
    capacity = 32
    tp = lax.axis_size("tp")
    share = capacity // tp
    slots = experts * share
    chosen = group_choice[None, :] * EPG + member_choice.T
    mine = lax.axis_index("tp").astype(jnp.int32).reshape(1)
    whole = pl.BlockSpec(memory_space=pltpu.VMEM)
    scalar = pl.BlockSpec(memory_space=pltpu.SMEM)
    outgoing, places = pl.pallas_call(
        dispatch_kernel,
        in_specs=[scalar, whole, whole, whole],
        out_specs=[whole, whole],
        out_shape=[
            jax.ShapeDtypeStruct((slots, width), bf16),
            jax.ShapeDtypeStruct((TOP, tokens, LANES), jnp.int32),
        ],
        scratch_shapes=[pltpu.VMEM((tokens, width), bf16)],
        name="dispatch",
    )(mine, chosen, moe_rows, norm_gain[None, :])
    incoming = lax.all_to_all(
        outgoing.reshape(experts, share * width // LANES, LANES), "ep", 0, 0, tiled=True
    )
    shared = incoming.reshape(slots, width).astype(jnp.float16)
    block_rows = lax.all_gather(shared, "tp", axis=0, tiled=True).astype(bf16)
    total = block_rows.shape[0]
    hidden = pl.pallas_call(
        hidden_kernel,
        in_specs=[whole, whole, whole],
        out_specs=whole,
        out_shape=jax.ShapeDtypeStruct((total + 16, w_gate.shape[2]), bf16),
        scratch_shapes=[pltpu.VMEM((total, w_gate.shape[2]), bf16)],
        name="hidden",
    )(block_rows, w_gate[0], w_up[0])
    spread = lax.all_gather(hidden.astype(jnp.float16), "tp", axis=0, tiled=False).astype(bf16)
    out_width = w_down.shape[2]
    produced = pl.pallas_call(
        down_kernel,
        in_specs=[whole, whole],
        out_specs=whole,
        out_shape=jax.ShapeDtypeStruct((total, out_width), bf16),
        name="down",
    )(spread, w_down[0])
    sources = lax.axis_size("ep")
    ordered = produced.reshape(tp, sources, share, out_width).transpose(1, 0, 2, 3)
    returned = lax.all_to_all(
        ordered.reshape(sources, capacity, out_width), "ep", 0, 0, tiled=True
    )
    return pl.pallas_call(
        combine_kernel,
        in_specs=[whole, whole, whole],
        out_specs=whole,
        out_shape=jax.ShapeDtypeStruct((tokens, out_width), bf16),
        name="combine",
    )(places, route_weight, returned.reshape(experts * capacity, out_width))


def shards(
    queries,
    keys_values,
    sink_logits,
    moe_rows,
    norm_gain,
    group_choice,
    member_choice,
    route_weight,
    w_gate,
    w_up,
    w_down,
):
    attended = attend_window(queries, keys_values, sink_logits)
    mixed = route_experts(
        moe_rows, norm_gain, group_choice, member_choice, route_weight, w_gate, w_up, w_down
    )
    return (attended, mixed)


def solution(mesh):
    in_specs = (
        P(("ep", "tp"), None),
        P(None, ("ep", "tp"), None),
        P(),
        P("ep", None),
        P(),
        P("ep"),
        P("ep", None),
        P("ep", None),
        P("ep", None, "tp"),
        P("ep", None, "tp"),
        P("ep", None, "tp"),
    )
    out_specs = (P(("ep", "tp"), None), P("ep", "tp"))
    return jax.shard_map(shards, mesh=mesh, in_specs=in_specs, out_specs=out_specs, check_vma=False)
```

```python
import jax
import jax.numpy as jnp
from jax import lax
from jax.experimental import pallas as pl
from jax.experimental.pallas import tpu as pltpu
from jax.sharding import PartitionSpec as P

QH = 16
KVH = 4
HD = 64
WINDOW = 128
EPG = 4
TOP = 2
LANES = 128
EXPERTS = 32
CAPACITY = 32
TP = 16
ROW_SCALE = 256.0
LEVELS = 11


def attention_kernel(first_ref, sink_ref, q_ref, prev_ref, cur_ref, edge_ref, out_ref):
    block = pl.program_id(0)
    f32 = jnp.float32
    bf16 = jnp.bfloat16
    row = lax.broadcasted_iota(jnp.int32, (WINDOW, WINDOW), 0)
    col = lax.broadcasted_iota(jnp.int32, (WINDOW, WINDOW), 1)
    causal = col <= row
    lane = lax.broadcasted_iota(jnp.int32, (WINDOW, LANES), 1)
    low = lane < HD
    at_start = block == 0
    hidden_prev = jnp.where(at_start, first_ref[0], 0)
    floor = jnp.where(hidden_prev == 1, f32(-1e30), f32(0.0))
    keep = jnp.where(hidden_prev == 1, f32(0.0), f32(1.0))
    zero = jnp.zeros((WINDOW, LANES), bf16)
    for c in range(KVH):
        lanes = pl.ds((c // 2) * LANES, LANES)
        mine = low if c % 2 == 0 else jnp.logical_not(low)
        parts = []
        for which in range(2):
            before = jnp.where(at_start, edge_ref[which, :, lanes], prev_ref[which, :, lanes])
            now = cur_ref[which, :, lanes]
            halves = []
            for value in (before, now):
                own = jnp.where(mine, value, zero)
                swapped = pltpu.roll(own.astype(f32), HD, 1).astype(bf16)
                halves.append((own, swapped) if c % 2 == 0 else (swapped, own))
            (a_prev, b_prev), (a_cur, b_cur) = halves
            parts.append(jnp.concatenate([a_prev, a_cur, b_prev, b_cur], axis=0))
        keys, values = parts
        keys = keys * bf16(HD ** (-0.5))
        for p in range(2):
            head = c * 4 + p * 2
            at = c * 256 + p * LANES
            q = q_ref[:, at : at + LANES]
            scores = lax.dot_general(q, keys, (((1,), (1,)), ((), ())), preferred_element_type=f32)
            pieces = []
            sums = []
            for side in range(2):
                base = side * 2 * WINDOW
                s_prev = scores[:, base : base + WINDOW] * keep + floor
                s_cur = scores[:, base + WINDOW : base + 2 * WINDOW]
                s = jnp.where(causal, s_cur, s_prev)
                sink = sink_ref[head + side]
                highest = jnp.maximum(jnp.max(s, axis=1, keepdims=True), sink)
                w = jnp.exp(s - highest)
                sums.append(jnp.sum(w, axis=1, keepdims=True) + jnp.exp(sink - highest))
                rounded = w.astype(bf16)
                pieces.append(jnp.where(causal, zero, rounded))
                pieces.append(jnp.where(causal, rounded, zero))
            weights = jnp.concatenate(pieces, axis=1)
            summed = jnp.dot(weights, values, preferred_element_type=f32)
            total = jnp.where(low, sums[0], sums[1])
            out_ref[:, at : at + LANES] = (summed / total).astype(bf16)


def edge_of(keys_values):
    length = keys_values.shape[1]
    peers = lax.axis_size(("ep", "tp"))
    pairs = [(i, i + 1) for i in range(peers - 1)]
    return lax.ppermute(keys_values[:, length - WINDOW :, :], ("ep", "tp"), pairs)


def attend_window(queries, keys_values, sink_logits, edge):
    blocks = queries.shape[0] // WINDOW
    width = keys_values.shape[2]
    first = (lax.axis_index(("ep", "tp")) == 0).astype(jnp.int32).reshape(1)
    return pl.pallas_call(
        attention_kernel,
        grid=(blocks,),
        in_specs=[
            pl.BlockSpec(memory_space=pltpu.SMEM),
            pl.BlockSpec(memory_space=pltpu.SMEM),
            pl.BlockSpec((WINDOW, queries.shape[1]), lambda b: (b, 0)),
            pl.BlockSpec((2, WINDOW, width), lambda b: (0, jnp.maximum(b - 1, 0), 0)),
            pl.BlockSpec((2, WINDOW, width), lambda b: (0, b, 0)),
            pl.BlockSpec((2, WINDOW, width), lambda b: (0, 0, 0)),
        ],
        out_specs=pl.BlockSpec((WINDOW, queries.shape[1]), lambda b: (b, 0)),
        out_shape=jax.ShapeDtypeStruct(queries.shape, jnp.bfloat16),
        cost_estimate=pl.CostEstimate(flops=3 * 10**9, bytes_accessed=3 * 10**6, transcendentals=10**6),
        name="attention",
    )(first, sink_logits, queries, keys_values, keys_values, edge)


def dispatch_kernel(mine_ref, group_ref, member_ref, rows_ref, gain_ref, out_ref, place_ref, normed_ref):
    f32 = jnp.float32
    bf16 = jnp.bfloat16
    tokens = rows_ref.shape[0]
    values = rows_ref[...].astype(f32)
    mean = jnp.mean(values * values, axis=1, keepdims=True)
    normed = (values * lax.rsqrt(mean + 1e-06) * gain_ref[...]).astype(bf16)
    normed_ref[...] = normed * bf16(ROW_SCALE)
    chosen = group_ref[...] * EPG + member_ref[...]
    which = lax.broadcasted_iota(jnp.int32, (EXPERTS, tokens), 0)
    first = (which == chosen[0:1, :]).astype(f32)
    second = (which == chosen[1:2, :]).astype(f32)
    before = (
        lax.broadcasted_iota(jnp.int32, (tokens, tokens), 0)
        < lax.broadcasted_iota(jnp.int32, (tokens, tokens), 1)
    ).astype(f32).astype(bf16)
    earlier = jnp.dot((first + second).astype(bf16), before, preferred_element_type=f32)
    places = []
    for k, hot in enumerate((first, second)):
        place = jnp.sum(hot * earlier, axis=0, keepdims=True).astype(jnp.int32)
        places.append(chosen[k : k + 1, :] * CAPACITY + place)
        place_ref[k : k + 1, :] = places[k]
    slots = out_ref.shape[0]
    share = slots // EXPERTS
    slot = lax.broadcasted_iota(jnp.int32, (slots, tokens), 0)
    wanted = (slot // share) * CAPACITY + mine_ref[0] * share + slot % share
    pick = ((places[0] == wanted) | (places[1] == wanted)).astype(f32).astype(bf16)
    out_ref[...] = jnp.dot(pick, normed_ref[...], preferred_element_type=f32).astype(bf16)


def prepare_kernel(place_ref, weight_ref, hot_ref, column_ref):
    f32 = jnp.float32
    bf16 = jnp.bfloat16
    tokens = place_ref.shape[1]
    slots = hot_ref.shape[2]
    for k in range(TOP):
        wide = jnp.broadcast_to(place_ref[k : k + 1, :].astype(f32), (LANES, tokens))
        place = wide.T.astype(jnp.int32)
        for j in range(slots // LANES):
            slot = lax.broadcasted_iota(jnp.int32, (tokens, LANES), 1) + j * LANES
            hot_ref[k, :, j * LANES : (j + 1) * LANES] = (place == slot).astype(f32).astype(bf16)
        column_ref[k] = jnp.broadcast_to(weight_ref[k : k + 1, :], (LANES, tokens)).T


def hidden_kernel(y_ref, out_ref, plain_ref, ordered_ref):
    f32 = jnp.float32
    bf16 = jnp.bfloat16
    rows, width = plain_ref.shape
    share = CAPACITY // TP
    sources = rows // CAPACITY
    back = f32(1.0 / ROW_SCALE)
    peak = jnp.zeros((8, width), f32)
    step = share * sources
    for i in range(TP):
        gate = y_ref[i * step : (i + 1) * step, :width] * back
        up = y_ref[i * step : (i + 1) * step, width:] * back
        hidden = (gate / (1.0 + jnp.exp(-gate)) * up).astype(bf16).astype(f32)
        plain_ref[i * step : (i + 1) * step, :] = hidden
        peak = jnp.maximum(peak, jnp.max(jnp.abs(hidden).reshape(step // 8, 8, width), axis=0))
    top = jnp.max(jnp.max(peak, axis=1, keepdims=True), axis=0, keepdims=True)
    index = jnp.zeros((1, 1), f32)
    scale = jnp.full((1, 1), 2.0**71, f32)
    for i in range(1, LEVELS):
        reached = top >= f32(2.0 ** (8 * i - 64))
        index = jnp.where(reached, f32(i), index)
        scale = jnp.where(reached, f32(2.0 ** (71 - 8 * i)), scale)
    for i in range(TP):
        for j in range(share):
            part = plain_ref[pl.ds(i * step + j, sources, stride=share), :]
            ordered_ref[pl.ds(i * share + j, sources, stride=CAPACITY), :] = part
    out_ref[:rows, :] = (ordered_ref[...] * scale).astype(bf16)
    out_ref[rows:, :] = jnp.broadcast_to(index, (16, width)).astype(bf16)


def combine_kernel(hot_ref, column_ref, rows_ref, out_ref):
    total = None
    for k in range(TOP):
        picked = jnp.dot(hot_ref[k], rows_ref[...], preferred_element_type=jnp.float32)
        part = column_ref[k] * picked
        total = part if total is None else total + part
    out_ref[...] = total.astype(jnp.bfloat16)


def near(value):
    return pltpu.with_memory_space_constraint(value, pltpu.VMEM)


def route_experts(
    moe_rows, norm_gain, group_choice, member_choice, route_weight, w_gate, w_up, w_down, edge
):
    bf16 = jnp.bfloat16
    tokens, width = moe_rows.shape
    share = CAPACITY // TP
    slots = EXPERTS * share
    mine = lax.axis_index("tp").astype(jnp.int32).reshape(1)
    whole = pl.BlockSpec(memory_space=pltpu.VMEM)
    scalar = pl.BlockSpec(memory_space=pltpu.SMEM)
    outgoing, places = pl.pallas_call(
        dispatch_kernel,
        in_specs=[scalar, whole, whole, whole, whole],
        out_specs=[whole, whole],
        out_shape=[
            pltpu.VMEM((slots, width), bf16),
            pltpu.VMEM((TOP, tokens), jnp.int32),
        ],
        scratch_shapes=[pltpu.VMEM((tokens, width), bf16)],
        name="dispatch",
    )(mine, group_choice[None, :], member_choice.T, moe_rows, norm_gain[None, :])
    incoming = lax.all_to_all(
        outgoing.reshape(EXPERTS, share * width // LANES, LANES), "ep", 0, 0, tiled=True
    )
    hots, columns = pl.pallas_call(
        prepare_kernel,
        in_specs=[whole, whole],
        out_specs=[whole, whole],
        out_shape=[
            pltpu.VMEM((TOP, tokens, EXPERTS * CAPACITY), bf16),
            pltpu.VMEM((TOP, tokens, LANES), jnp.float32),
        ],
        name="prepare",
    )(places, route_weight.T)
    both = jnp.concatenate([w_gate[0], w_up[0]], axis=1)
    incoming, edge, hots, columns, both = lax.optimization_barrier(
        (incoming, edge, hots, columns, both)
    )
    shared = incoming.reshape(slots, width).astype(jnp.float16)
    block_rows = lax.all_gather(shared, "tp", axis=0, tiled=True).astype(bf16)
    total = block_rows.shape[0]
    y = jnp.dot(block_rows, both, preferred_element_type=jnp.float32)
    units = w_gate.shape[2]
    hidden = pl.pallas_call(
        hidden_kernel,
        in_specs=[whole],
        out_specs=whole,
        out_shape=pltpu.VMEM((total + 16, units), bf16),
        scratch_shapes=[pltpu.VMEM((total, units), jnp.float32)] * 2,
        name="hidden",
    )(near(y))
    spread = lax.all_gather(hidden.astype(jnp.float16), "tp", axis=0, tiled=False)
    index = spread[:, total, 0].astype(jnp.float32)
    factor = jnp.full(index.shape, 2.0**-71, jnp.float32)
    for i in range(1, LEVELS):
        factor = jnp.where(index == i, 2.0 ** (8 * i - 71), factor)
    out_width = w_down.shape[2]
    weight = w_down[0].reshape(TP, units, out_width).astype(jnp.float32) * factor[:, None, None]
    produced = jnp.einsum(
        "trk,tko->ro",
        spread.astype(bf16),
        weight.astype(bf16),
        preferred_element_type=jnp.float32,
    ).astype(bf16)[:total]
    returned = lax.all_to_all(
        produced.reshape(total // CAPACITY, CAPACITY, out_width), "ep", 0, 0, tiled=True
    )
    mixed = pl.pallas_call(
        combine_kernel,
        in_specs=[whole, whole, whole],
        out_specs=whole,
        out_shape=jax.ShapeDtypeStruct((tokens, out_width), bf16),
        name="combine",
    )(near(hots), near(columns), near(returned.reshape(EXPERTS * CAPACITY, out_width)))
    return mixed, edge, produced


def shards(
    queries,
    keys_values,
    sink_logits,
    moe_rows,
    norm_gain,
    group_choice,
    member_choice,
    route_weight,
    w_gate,
    w_up,
    w_down,
):
    edge = edge_of(keys_values)
    mixed, edge, produced = route_experts(
        moe_rows,
        norm_gain,
        group_choice,
        member_choice,
        route_weight,
        w_gate,
        w_up,
        w_down,
        edge,
    )
    sink_logits, produced = lax.optimization_barrier((sink_logits, produced))
    attended = attend_window(queries, keys_values, sink_logits, edge)
    return (attended, mixed)


def solution(mesh):
    in_specs = (
        P(("ep", "tp"), None),
        P(None, ("ep", "tp"), None),
        P(),
        P("ep", None),
        P(),
        P("ep"),
        P("ep", None),
        P("ep", None),
        P("ep", None, "tp"),
        P("ep", None, "tp"),
        P("ep", None, "tp"),
    )
    out_specs = (P(("ep", "tp"), None), P("ep", "tp"))
    return jax.shard_map(shards, mesh=mesh, in_specs=in_specs, out_specs=out_specs, check_vma=False)
```

```python
import jax
import jax.numpy as jnp
from jax import lax
from jax.experimental import pallas as pl
from jax.experimental.pallas import tpu as pltpu
from jax.sharding import PartitionSpec as P

QH = 16
KVH = 4
HD = 64
WINDOW = 128
EPG = 4
TOP = 2
LANES = 128
EXPERTS = 32
CAPACITY = 32
TP = 16
ROW_SCALE = 256.0
LEVELS = 11


def near(value):
    return pltpu.with_memory_space_constraint(value, pltpu.VMEM)


def attention_kernel(first_ref, sink_ref, q_ref, kv_ref, edge_ref, out_ref, band_ref):
    f32 = jnp.float32
    bf16 = jnp.bfloat16
    blocks = q_ref.shape[0] // WINDOW
    row = lax.broadcasted_iota(jnp.int32, (WINDOW, WINDOW), 0)
    col = lax.broadcasted_iota(jnp.int32, (WINDOW, WINDOW), 1)
    causal = col <= row
    low = lax.broadcasted_iota(jnp.int32, (WINDOW, LANES), 1) < HD
    zero = jnp.zeros((WINDOW, LANES), bf16)
    for which in range(2):
        for part in range(blocks + 1):
            for h in range(KVH // 2):
                lanes = slice(h * LANES, (h + 1) * LANES)
                if part == 0:
                    value = edge_ref[which, :, lanes]
                else:
                    value = kv_ref[which, (part - 1) * WINDOW : part * WINDOW, lanes]
                if which == 0:
                    value = value * bf16(HD ** (-0.5))
                turned = pltpu.roll(value.astype(f32), HD, 1).astype(bf16)
                at = slice(part * WINDOW, (part + 1) * WINDOW)
                band_ref[which, 2 * h, 0, at, :] = jnp.where(low, value, zero)
                band_ref[which, 2 * h, 1, at, :] = jnp.where(low, zero, turned)
                band_ref[which, 2 * h + 1, 0, at, :] = jnp.where(low, turned, zero)
                band_ref[which, 2 * h + 1, 1, at, :] = jnp.where(low, zero, value)

    absent = jnp.where(first_ref[0] == 1, f32(-1e30), f32(0.0))
    bias = jnp.where(causal, f32(0.0), absent)
    for block in range(blocks):
        start = block * WINDOW
        band = pl.ds(start, 2 * WINDOW)
        for c in range(KVH):
            keys = jnp.concatenate([band_ref[0, c, 0, band, :], band_ref[0, c, 1, band, :]], axis=0)
            values = jnp.concatenate([band_ref[1, c, 0, band, :], band_ref[1, c, 1, band, :]], axis=0)
            q = jnp.concatenate(
                [q_ref[pl.ds(start, WINDOW), c * 256 + p * LANES : c * 256 + (p + 1) * LANES] for p in range(2)],
                axis=0,
            )
            scores = lax.dot_general(q, keys, (((1,), (1,)), ((), ())), preferred_element_type=f32)
            lines = []
            totals = []
            for p in range(2):
                head = c * 4 + p * 2
                pieces = []
                sums = []
                tops = []
                for side in range(2):
                    base = side * 2 * WINDOW
                    s_prev = scores[p * WINDOW : (p + 1) * WINDOW, base : base + WINDOW]
                    s_cur = scores[p * WINDOW : (p + 1) * WINDOW, base + WINDOW : base + 2 * WINDOW]
                    s = jnp.where(causal, s_cur, s_prev)
                    if block == 0:
                        s = s + bias
                    highest = jnp.maximum(jnp.max(s, axis=1, keepdims=True), sink_ref[head + side])
                    w = jnp.exp(s - highest)
                    sums.append(jnp.sum(w, axis=1, keepdims=True))
                    tops.append(highest)
                    rounded = w.astype(bf16)
                    pieces.append(jnp.where(causal, zero, rounded))
                    pieces.append(jnp.where(causal, rounded, zero))
                lines.append(jnp.concatenate(pieces, axis=1))
                sink = jnp.where(low, sink_ref[head], sink_ref[head + 1])
                rest = jnp.exp(sink - jnp.where(low, tops[0], tops[1]))
                totals.append(jnp.where(low, sums[0], sums[1]) + rest)
            summed = jnp.dot(jnp.concatenate(lines, axis=0), values, preferred_element_type=f32)
            for p in range(2):
                at = c * 256 + p * LANES
                out_ref[pl.ds(start, WINDOW), at : at + LANES] = (
                    summed[p * WINDOW : (p + 1) * WINDOW] / totals[p]
                ).astype(bf16)


def edge_of(keys_values):
    length = keys_values.shape[1]
    peers = lax.axis_size(("ep", "tp"))
    pairs = [(i, i + 1) for i in range(peers - 1)]
    return lax.ppermute(keys_values[:, length - WINDOW :, :], ("ep", "tp"), pairs)


def attend_window(queries, keys_values, sink_logits, edge):
    first = (lax.axis_index(("ep", "tp")) == 0).astype(jnp.int32).reshape(1)
    whole = pl.BlockSpec(memory_space=pltpu.VMEM)
    scalar = pl.BlockSpec(memory_space=pltpu.SMEM)
    rows = keys_values.shape[1] + WINDOW
    return pl.pallas_call(
        attention_kernel,
        in_specs=[scalar, scalar, whole, whole, whole],
        out_specs=whole,
        out_shape=jax.ShapeDtypeStruct(queries.shape, jnp.bfloat16),
        scratch_shapes=[pltpu.VMEM((2, KVH, 2, rows, LANES), jnp.bfloat16)],
        cost_estimate=pl.CostEstimate(flops=3 * 10**9, bytes_accessed=3 * 10**6, transcendentals=10**6),
        name="attention",
    )(first, sink_logits, near(queries), near(keys_values), near(edge))


def dispatch_kernel(mine_ref, group_ref, member_ref, rows_ref, gain_ref, out_ref, place_ref, normed_ref, line_ref):
    f32 = jnp.float32
    bf16 = jnp.bfloat16
    tokens, width = rows_ref.shape
    pieces = width // LANES
    values = rows_ref[...].astype(f32)
    mean = jnp.mean(values * values, axis=1, keepdims=True)
    normed = (values * lax.rsqrt(mean + 1e-06) * gain_ref[...]).astype(bf16)
    normed_ref[...] = normed * bf16(ROW_SCALE)
    chosen = group_ref[...] * EPG + member_ref[...]
    which = lax.broadcasted_iota(jnp.int32, (EXPERTS, tokens), 0)
    first = (which == chosen[0:1, :]).astype(f32)
    second = (which == chosen[1:2, :]).astype(f32)
    before = (
        lax.broadcasted_iota(jnp.int32, (tokens, tokens), 0)
        < lax.broadcasted_iota(jnp.int32, (tokens, tokens), 1)
    ).astype(f32).astype(bf16)
    earlier = jnp.dot((first + second).astype(bf16), before, preferred_element_type=f32)
    places = []
    for k, hot in enumerate((first, second)):
        place = jnp.sum(hot * earlier, axis=0, keepdims=True).astype(jnp.int32)
        places.append(chosen[k : k + 1, :] * CAPACITY + place)
        place_ref[k : k + 1, :] = places[k]
    share = CAPACITY // TP
    slots = EXPERTS * share
    slot = lax.broadcasted_iota(jnp.int32, (slots, tokens), 0)
    wanted = (slot // share) * CAPACITY + mine_ref[0] * share + slot % share
    pick = ((places[0] == wanted) | (places[1] == wanted)).astype(f32).astype(bf16)
    picked = jnp.dot(pick, normed_ref[...], preferred_element_type=f32)
    for j in range(pieces):
        line_ref[pl.ds(j, slots, stride=pieces), :] = picked[:, j * LANES : (j + 1) * LANES]
    out_ref[...] = line_ref[...].reshape(out_ref.shape).astype(bf16)


def prepare_kernel(place_ref, weight_ref, hot_ref, column_ref):
    f32 = jnp.float32
    bf16 = jnp.bfloat16
    tokens = place_ref.shape[1]
    slots = hot_ref.shape[2]
    for k in range(TOP):
        wide = jnp.broadcast_to(place_ref[k : k + 1, :].astype(f32), (LANES, tokens))
        place = wide.T.astype(jnp.int32)
        for j in range(slots // LANES):
            slot = lax.broadcasted_iota(jnp.int32, (tokens, LANES), 1) + j * LANES
            hot_ref[k, :, j * LANES : (j + 1) * LANES] = (place == slot).astype(f32).astype(bf16)
        column_ref[k] = jnp.broadcast_to(weight_ref[k : k + 1, :], (LANES, tokens)).T


def hidden_kernel(y_ref, out_ref, plain_ref, ordered_ref):
    f32 = jnp.float32
    bf16 = jnp.bfloat16
    rows, width = plain_ref.shape
    share = CAPACITY // TP
    sources = rows // CAPACITY
    back = f32(1.0 / ROW_SCALE)
    peak = jnp.zeros((8, width), f32)
    step = share * sources
    for i in range(TP):
        gate = y_ref[i * step : (i + 1) * step, :width] * back
        up = y_ref[i * step : (i + 1) * step, width:] * back
        hidden = (gate / (1.0 + jnp.exp(-gate)) * up).astype(bf16).astype(f32)
        plain_ref[i * step : (i + 1) * step, :] = hidden
        peak = jnp.maximum(peak, jnp.max(jnp.abs(hidden).reshape(step // 8, 8, width), axis=0))
    top = jnp.max(jnp.max(peak, axis=1, keepdims=True), axis=0, keepdims=True)
    index = jnp.zeros((1, 1), f32)
    scale = jnp.full((1, 1), 2.0**71, f32)
    for i in range(1, LEVELS):
        reached = top >= f32(2.0 ** (8 * i - 64))
        index = jnp.where(reached, f32(i), index)
        scale = jnp.where(reached, f32(2.0 ** (71 - 8 * i)), scale)
    for i in range(TP):
        for j in range(share):
            part = plain_ref[pl.ds(i * step + j, sources, stride=share), :]
            ordered_ref[pl.ds(i * share + j, sources, stride=CAPACITY), :] = part
    out_ref[:rows, :] = (ordered_ref[...] * scale).astype(bf16)
    out_ref[rows:, :] = jnp.broadcast_to(index, (16, width)).astype(bf16)


def combine_kernel(hot_ref, column_ref, rows_ref, out_ref):
    total = None
    for k in range(TOP):
        picked = jnp.dot(hot_ref[k], rows_ref[...], preferred_element_type=jnp.float32)
        part = column_ref[k] * picked
        total = part if total is None else total + part
    out_ref[...] = total.astype(jnp.bfloat16)


def route_experts(
    moe_rows, norm_gain, group_choice, member_choice, route_weight, w_gate, w_up, w_down, edge
):
    bf16 = jnp.bfloat16
    tokens, width = moe_rows.shape
    share = CAPACITY // TP
    slots = EXPERTS * share
    mine = lax.axis_index("tp").astype(jnp.int32).reshape(1)
    whole = pl.BlockSpec(memory_space=pltpu.VMEM)
    scalar = pl.BlockSpec(memory_space=pltpu.SMEM)
    outgoing, places = pl.pallas_call(
        dispatch_kernel,
        in_specs=[scalar, whole, whole, whole, whole],
        out_specs=[whole, whole],
        out_shape=[
            jax.ShapeDtypeStruct((EXPERTS, share * width // LANES, LANES), bf16),
            pltpu.VMEM((TOP, tokens), jnp.int32),
        ],
        scratch_shapes=[
            pltpu.VMEM((tokens, width), bf16),
            pltpu.VMEM((slots * width // LANES, LANES), jnp.float32),
        ],
        name="dispatch",
    )(mine, group_choice[None, :], member_choice.T, moe_rows, norm_gain[None, :])
    incoming = lax.all_to_all(outgoing, "ep", 0, 0, tiled=True)
    hots, columns = pl.pallas_call(
        prepare_kernel,
        in_specs=[whole, whole],
        out_specs=[whole, whole],
        out_shape=[
            pltpu.VMEM((TOP, tokens, EXPERTS * CAPACITY), bf16),
            pltpu.VMEM((TOP, tokens, LANES), jnp.float32),
        ],
        name="prepare",
    )(places, route_weight.T)
    both = jnp.concatenate([w_gate[0], w_up[0]], axis=1)
    incoming, edge, hots, columns, both = lax.optimization_barrier(
        (incoming, edge, hots, columns, both)
    )
    shared = incoming.reshape(slots, width).astype(jnp.float16)
    block_rows = lax.all_gather(shared, "tp", axis=0, tiled=True).astype(bf16)
    total = block_rows.shape[0]
    y = jnp.dot(block_rows, both, preferred_element_type=jnp.float32)
    units = w_gate.shape[2]
    hidden = pl.pallas_call(
        hidden_kernel,
        in_specs=[whole],
        out_specs=whole,
        out_shape=pltpu.VMEM((total + 16, units), bf16),
        scratch_shapes=[pltpu.VMEM((total, units), jnp.float32)] * 2,
        name="hidden",
    )(near(y))
    spread = lax.all_gather(hidden.astype(jnp.float16), "tp", axis=0, tiled=False)
    index = spread[:, total, 0].astype(jnp.float32)
    factor = jnp.full(index.shape, 2.0**-71, jnp.float32)
    for i in range(1, LEVELS):
        factor = jnp.where(index == i, 2.0 ** (8 * i - 71), factor)
    out_width = w_down.shape[2]
    weight = w_down[0].reshape(TP, units, out_width).astype(jnp.float32) * factor[:, None, None]
    produced = jnp.einsum(
        "trk,tko->ro",
        spread.astype(bf16),
        weight.astype(bf16),
        preferred_element_type=jnp.float32,
    ).astype(bf16)[:total]
    returned = lax.all_to_all(
        produced.reshape(total // CAPACITY, CAPACITY, out_width), "ep", 0, 0, tiled=True
    )
    mixed = pl.pallas_call(
        combine_kernel,
        in_specs=[whole, whole, whole],
        out_specs=whole,
        out_shape=jax.ShapeDtypeStruct((tokens, out_width), bf16),
        name="combine",
    )(near(hots), near(columns), near(returned.reshape(EXPERTS * CAPACITY, out_width)))
    return mixed, edge, produced


def shards(
    queries,
    keys_values,
    sink_logits,
    moe_rows,
    norm_gain,
    group_choice,
    member_choice,
    route_weight,
    w_gate,
    w_up,
    w_down,
):
    edge = edge_of(keys_values)
    mixed, edge, produced = route_experts(
        moe_rows,
        norm_gain,
        group_choice,
        member_choice,
        route_weight,
        w_gate,
        w_up,
        w_down,
        edge,
    )
    sink_logits, produced = lax.optimization_barrier((sink_logits, produced))
    attended = attend_window(queries, keys_values, sink_logits, edge)
    return (attended, mixed)


def solution(mesh):
    in_specs = (
        P(("ep", "tp"), None),
        P(None, ("ep", "tp"), None),
        P(),
        P("ep", None),
        P(),
        P("ep"),
        P("ep", None),
        P("ep", None),
        P("ep", None, "tp"),
        P("ep", None, "tp"),
        P("ep", None, "tp"),
    )
    out_specs = (P(("ep", "tp"), None), P("ep", "tp"))
    return jax.shard_map(shards, mesh=mesh, in_specs=in_specs, out_specs=out_specs, check_vma=False)
```

```python
import jax
import jax.numpy as jnp
from jax import lax
from jax.experimental import pallas as pl
from jax.experimental.pallas import tpu as pltpu
from jax.sharding import PartitionSpec as P


KVH = 4
HD = 64
WINDOW = 128
EPG = 4
TOP = 2
LANES = 128
EXPERTS = 32
CAPACITY = 32
TP = 16
ROW_SCALE = 256.0
LEVELS = 11


def near(value):
    return pltpu.with_memory_space_constraint(value, pltpu.VMEM)


def attention_kernel(first_ref, sink_ref, q_ref, kv_ref, edge_ref, out_ref, band_ref):
    f32 = jnp.float32
    bf16 = jnp.bfloat16
    blocks = q_ref.shape[0] // WINDOW
    row = lax.broadcasted_iota(jnp.int32, (WINDOW, WINDOW), 0)
    col = lax.broadcasted_iota(jnp.int32, (WINDOW, WINDOW), 1)
    causal = col <= row
    low = lax.broadcasted_iota(jnp.int32, (WINDOW, LANES), 1) < HD
    zero = jnp.zeros((WINDOW, LANES), bf16)
    for which in range(2):
        for part in range(blocks + 1):
            for h in range(KVH // 2):
                lanes = slice(h * LANES, (h + 1) * LANES)
                if part == 0:
                    value = edge_ref[which, :, lanes]
                else:
                    value = kv_ref[which, (part - 1) * WINDOW : part * WINDOW, lanes]
                if which == 0:
                    value = value * bf16(HD ** (-0.5))
                turned = pltpu.roll(value.astype(f32), HD, 1).astype(bf16)
                at = slice(part * WINDOW, (part + 1) * WINDOW)
                band_ref[which, 2 * h, 0, at, :] = jnp.where(low, value, zero)
                band_ref[which, 2 * h, 1, at, :] = jnp.where(low, zero, turned)
                band_ref[which, 2 * h + 1, 0, at, :] = jnp.where(low, turned, zero)
                band_ref[which, 2 * h + 1, 1, at, :] = jnp.where(low, zero, value)

    absent = jnp.where(first_ref[0] == 1, f32(-1e30), f32(0.0))
    bias = jnp.where(causal, f32(0.0), absent)
    for block in range(blocks):
        start = block * WINDOW
        band = pl.ds(start, 2 * WINDOW)
        for c in range(KVH):
            keys = jnp.concatenate([band_ref[0, c, 0, band, :], band_ref[0, c, 1, band, :]], axis=0)
            values = jnp.concatenate([band_ref[1, c, 0, band, :], band_ref[1, c, 1, band, :]], axis=0)
            q = jnp.concatenate(
                [q_ref[pl.ds(start, WINDOW), c * 256 + p * LANES : c * 256 + (p + 1) * LANES] for p in range(2)],
                axis=0,
            )
            scores = lax.dot_general(q, keys, (((1,), (1,)), ((), ())), preferred_element_type=f32)
            lines = []
            totals = []
            for p in range(2):
                head = c * 4 + p * 2
                pieces = []
                sums = []
                tops = []
                for side in range(2):
                    base = side * 2 * WINDOW
                    s_prev = scores[p * WINDOW : (p + 1) * WINDOW, base : base + WINDOW]
                    s_cur = scores[p * WINDOW : (p + 1) * WINDOW, base + WINDOW : base + 2 * WINDOW]
                    s = jnp.where(causal, s_cur, s_prev)
                    if block == 0:
                        s = s + bias
                    highest = jnp.maximum(jnp.max(s, axis=1, keepdims=True), sink_ref[head + side])
                    w = jnp.exp(s - highest)
                    sums.append(jnp.sum(w, axis=1, keepdims=True))
                    tops.append(highest)
                    rounded = w.astype(bf16)
                    pieces.append(jnp.where(causal, zero, rounded))
                    pieces.append(jnp.where(causal, rounded, zero))
                lines.append(jnp.concatenate(pieces, axis=1))
                sink = jnp.where(low, sink_ref[head], sink_ref[head + 1])
                rest = jnp.exp(sink - jnp.where(low, tops[0], tops[1]))
                totals.append(jnp.where(low, sums[0], sums[1]) + rest)
            summed = jnp.dot(jnp.concatenate(lines, axis=0), values, preferred_element_type=f32)
            for p in range(2):
                at = c * 256 + p * LANES
                out_ref[pl.ds(start, WINDOW), at : at + LANES] = (
                    summed[p * WINDOW : (p + 1) * WINDOW] / totals[p]
                ).astype(bf16)


def passed_along(value):
    peers = lax.axis_size(("ep", "tp"))
    pairs = [(i, i + 1) for i in range(peers - 1)]
    return lax.ppermute(value, ("ep", "tp"), pairs)


def attend_window(queries, keys_values, sink_logits, edge):
    first = (lax.axis_index(("ep", "tp")) == 0).astype(jnp.int32).reshape(1)
    whole = pl.BlockSpec(memory_space=pltpu.VMEM)
    scalar = pl.BlockSpec(memory_space=pltpu.SMEM)
    rows = keys_values.shape[1] + WINDOW
    return pl.pallas_call(
        attention_kernel,
        in_specs=[scalar, scalar, whole, whole, whole],
        out_specs=whole,
        out_shape=jax.ShapeDtypeStruct(queries.shape, jnp.bfloat16),
        scratch_shapes=[pltpu.VMEM((2, KVH, 2, rows, LANES), jnp.bfloat16)],
        cost_estimate=pl.CostEstimate(flops=3 * 10**9, bytes_accessed=3 * 10**6, transcendentals=10**6),
        name="attention",
    )(first, sink_logits, near(queries), near(keys_values), near(edge))


def dispatch_kernel(mine_ref, group_ref, member_ref, rows_ref, gain_ref, out_ref, place_ref, normed_ref, line_ref):
    f32 = jnp.float32
    bf16 = jnp.bfloat16
    tokens, width = rows_ref.shape
    pieces = width // LANES
    values = rows_ref[...].astype(f32)
    mean = jnp.mean(values * values, axis=1, keepdims=True)
    normed = (values * lax.rsqrt(mean + 1e-06) * gain_ref[...]).astype(bf16)
    normed_ref[...] = normed * bf16(ROW_SCALE)
    chosen = group_ref[...] * EPG + member_ref[...]
    which = lax.broadcasted_iota(jnp.int32, (EXPERTS, tokens), 0)
    first = (which == chosen[0:1, :]).astype(f32)
    second = (which == chosen[1:2, :]).astype(f32)
    before = (
        lax.broadcasted_iota(jnp.int32, (tokens, tokens), 0)
        < lax.broadcasted_iota(jnp.int32, (tokens, tokens), 1)
    ).astype(f32).astype(bf16)
    earlier = jnp.dot((first + second).astype(bf16), before, preferred_element_type=f32)
    places = []
    for k, hot in enumerate((first, second)):
        place = jnp.sum(hot * earlier, axis=0, keepdims=True).astype(jnp.int32)
        places.append(chosen[k : k + 1, :] * CAPACITY + place)
        place_ref[k : k + 1, :] = places[k]
    share = CAPACITY // TP
    slots = EXPERTS * share
    slot = lax.broadcasted_iota(jnp.int32, (slots, tokens), 0)
    wanted = (slot // share) * CAPACITY + mine_ref[0] * share + slot % share
    pick = ((places[0] == wanted) | (places[1] == wanted)).astype(f32).astype(bf16)
    picked = jnp.dot(pick, normed_ref[...], preferred_element_type=f32)
    for j in range(pieces):
        line_ref[pl.ds(j, slots, stride=pieces), :] = picked[:, j * LANES : (j + 1) * LANES]
    out_ref[...] = line_ref[...].reshape(out_ref.shape).astype(bf16)


def prepare_kernel(
    place_ref, weight_ref, gate_ref, up_ref, hot_ref, column_ref, both_ref, gate_sem, up_sem
):
    units = gate_ref.shape[1]
    gate_copy = pltpu.make_async_copy(gate_ref, both_ref.at[:, :units], gate_sem)
    up_copy = pltpu.make_async_copy(up_ref, both_ref.at[:, units:], up_sem)
    gate_copy.start()
    up_copy.start()
    f32 = jnp.float32
    bf16 = jnp.bfloat16
    tokens = place_ref.shape[1]
    slots = hot_ref.shape[2]
    for k in range(TOP):
        wide = jnp.broadcast_to(place_ref[k : k + 1, :].astype(f32), (LANES, tokens))
        place = wide.T.astype(jnp.int32)
        for j in range(slots // LANES):
            slot = lax.broadcasted_iota(jnp.int32, (tokens, LANES), 1) + j * LANES
            hot_ref[k, :, j * LANES : (j + 1) * LANES] = (place == slot).astype(f32).astype(bf16)
        column_ref[k] = jnp.broadcast_to(weight_ref[k : k + 1, :], (LANES, tokens)).T
    gate_copy.wait()
    up_copy.wait()


def hidden_kernel(y_ref, out_ref, plain_ref, ordered_ref):
    f32 = jnp.float32
    bf16 = jnp.bfloat16
    rows, width = plain_ref.shape
    share = CAPACITY // TP
    sources = rows // CAPACITY
    back = f32(1.0 / ROW_SCALE)
    peak = jnp.zeros((8, width), f32)
    step = share * sources
    for i in range(TP):
        gate = y_ref[i * step : (i + 1) * step, :width] * back
        up = y_ref[i * step : (i + 1) * step, width:] * back
        hidden = (gate / (1.0 + jnp.exp(-gate)) * up).astype(bf16).astype(f32)
        plain_ref[i * step : (i + 1) * step, :] = hidden
        peak = jnp.maximum(peak, jnp.max(jnp.abs(hidden).reshape(step // 8, 8, width), axis=0))
    top = jnp.max(jnp.max(peak, axis=1, keepdims=True), axis=0, keepdims=True)
    index = jnp.zeros((1, 1), f32)
    scale = jnp.full((1, 1), 2.0**71, f32)
    for i in range(1, LEVELS):
        reached = top >= f32(2.0 ** (8 * i - 64))
        index = jnp.where(reached, f32(i), index)
        scale = jnp.where(reached, f32(2.0 ** (71 - 8 * i)), scale)
    for i in range(TP):
        for j in range(share):
            part = plain_ref[pl.ds(i * step + j, sources, stride=share), :]
            ordered_ref[pl.ds(i * share + j, sources, stride=CAPACITY), :] = part
    out_ref[:rows, :] = (ordered_ref[...] * scale).astype(bf16)
    out_ref[rows:, :] = jnp.broadcast_to(index, (16, width)).astype(bf16)


def combine_kernel(hot_ref, column_ref, rows_ref, out_ref):
    total = None
    for k in range(TOP):
        picked = jnp.dot(hot_ref[k], rows_ref[...], preferred_element_type=jnp.float32)
        part = column_ref[k] * picked
        total = part if total is None else total + part
    out_ref[...] = total.astype(jnp.bfloat16)


def route_experts(
    moe_rows, norm_gain, group_choice, member_choice, route_weight, w_gate, w_up, w_down
):
    bf16 = jnp.bfloat16
    tokens, width = moe_rows.shape
    share = CAPACITY // TP
    slots = EXPERTS * share
    mine = lax.axis_index("tp").astype(jnp.int32).reshape(1)
    whole = pl.BlockSpec(memory_space=pltpu.VMEM)
    scalar = pl.BlockSpec(memory_space=pltpu.SMEM)
    outside = pl.BlockSpec(memory_space=pl.ANY)
    outgoing, places = pl.pallas_call(
        dispatch_kernel,
        in_specs=[scalar, whole, whole, whole, whole],
        out_specs=[whole, whole],
        out_shape=[
            jax.ShapeDtypeStruct((EXPERTS, share * width // LANES, LANES), bf16),
            pltpu.VMEM((TOP, tokens), jnp.int32),
        ],
        scratch_shapes=[
            pltpu.VMEM((tokens, width), bf16),
            pltpu.VMEM((slots * width // LANES, LANES), jnp.float32),
        ],
        name="dispatch",
    )(mine, group_choice[None, :], member_choice.T, moe_rows, norm_gain[None, :])
    incoming = lax.all_to_all(outgoing, "ep", 0, 0, tiled=True)
    hots, columns, both = pl.pallas_call(
        prepare_kernel,
        in_specs=[whole, whole, outside, outside],
        out_specs=[whole, whole, whole],
        out_shape=[
            pltpu.VMEM((TOP, tokens, EXPERTS * CAPACITY), bf16),
            pltpu.VMEM((TOP, tokens, LANES), jnp.float32),
            pltpu.VMEM((width, 2 * w_gate.shape[2]), bf16),
        ],
        scratch_shapes=[pltpu.SemaphoreType.DMA, pltpu.SemaphoreType.DMA],
        name="prepare",
    )(near(places), route_weight.T, w_gate[0], w_up[0])
    incoming, hots, columns, both = lax.optimization_barrier((incoming, hots, columns, both))
    shared = incoming.reshape(slots, width).astype(jnp.float16)
    block_rows = lax.all_gather(shared, "tp", axis=0, tiled=True).astype(bf16)
    total = block_rows.shape[0]
    y = jnp.dot(block_rows, both, preferred_element_type=jnp.float32)
    units = w_gate.shape[2]
    hidden = pl.pallas_call(
        hidden_kernel,
        in_specs=[whole],
        out_specs=whole,
        out_shape=pltpu.VMEM((total + 16, units), bf16),
        scratch_shapes=[pltpu.VMEM((total, units), jnp.float32)] * 2,
        name="hidden",
    )(near(y))
    spread = lax.all_gather(hidden.astype(jnp.float16), "tp", axis=0, tiled=False)
    index = spread[:, total, 0].astype(jnp.float32)
    factor = jnp.full(index.shape, 2.0**-71, jnp.float32)
    for i in range(1, LEVELS):
        factor = jnp.where(index == i, 2.0 ** (8 * i - 71), factor)
    out_width = w_down.shape[2]
    weight = w_down[0].reshape(TP, units, out_width).astype(jnp.float32) * factor[:, None, None]
    produced = jnp.einsum(
        "trk,tko->ro",
        spread[:, :total].astype(bf16),
        weight.astype(bf16),
        preferred_element_type=jnp.float32,
    ).astype(bf16)
    returned = lax.all_to_all(
        produced.reshape(total // CAPACITY, CAPACITY, out_width), "ep", 0, 0, tiled=True
    )
    mixed = pl.pallas_call(
        combine_kernel,
        in_specs=[whole, whole, whole],
        out_specs=whole,
        out_shape=jax.ShapeDtypeStruct((tokens, out_width), bf16),
        name="combine",
    )(near(hots), near(columns), near(returned.reshape(EXPERTS * CAPACITY, out_width)))
    return mixed, produced


def shards(
    queries,
    keys_values,
    sink_logits,
    moe_rows,
    norm_gain,
    group_choice,
    member_choice,
    route_weight,
    w_gate,
    w_up,
    w_down,
):
    edge = passed_along(keys_values[:, keys_values.shape[1] - WINDOW :, :])
    mixed, produced = route_experts(
        moe_rows,
        norm_gain,
        group_choice,
        member_choice,
        route_weight,
        w_gate,
        w_up,
        w_down,
    )
    sink_logits, produced = lax.optimization_barrier((sink_logits, produced))
    attended = attend_window(queries, keys_values, sink_logits, edge)
    return (attended, mixed)


def solution(mesh):
    in_specs = (
        P(("ep", "tp"), None),
        P(None, ("ep", "tp"), None),
        P(),
        P("ep", None),
        P(),
        P("ep"),
        P("ep", None),
        P("ep", None),
        P("ep", None, "tp"),
        P("ep", None, "tp"),
        P("ep", None, "tp"),
    )
    out_specs = (P(("ep", "tp"), None), P("ep", "tp"))
    return jax.shard_map(shards, mesh=mesh, in_specs=in_specs, out_specs=out_specs, check_vma=False)
```

```python
import jax
import jax.numpy as jnp
from jax import lax
from jax.experimental import pallas as pl
from jax.experimental.pallas import tpu as pltpu
from jax.sharding import PartitionSpec as P


KVH = 4
HD = 64
WINDOW = 128
EPG = 4
TOP = 2
LANES = 128
EXPERTS = 32
CAPACITY = 32
TP = 16
ROW_SCALE = 256.0
LEVELS = 11


def near(value):
    return pltpu.with_memory_space_constraint(value, pltpu.VMEM)


def attend_blocks(
    begin, blocks, first_ref, sink_ref, q_ref, kv_ref, edge_ref, out_ref, band_ref, done_ref, copy_sem
):
    f32 = jnp.float32
    bf16 = jnp.bfloat16
    row = lax.broadcasted_iota(jnp.int32, (WINDOW, WINDOW), 0)
    col = lax.broadcasted_iota(jnp.int32, (WINDOW, WINDOW), 1)
    causal = col <= row
    low = lax.broadcasted_iota(jnp.int32, (WINDOW, LANES), 1) < HD
    zero = jnp.zeros((WINDOW, LANES), bf16)
    for which in range(2):
        for part in range(blocks + 1):
            for h in range(KVH // 2):
                lanes = slice(h * LANES, (h + 1) * LANES)
                if part == 0 and edge_ref is not None:
                    value = edge_ref[which, :, lanes]
                else:
                    at = begin + part - 1
                    value = kv_ref[which, at * WINDOW : (at + 1) * WINDOW, lanes]
                if which == 0:
                    value = value * bf16(HD ** (-0.5))
                turned = pltpu.roll(value.astype(f32), HD, 1).astype(bf16)
                at = slice(part * WINDOW, (part + 1) * WINDOW)
                band_ref[which, 2 * h, 0, at, :] = jnp.where(low, value, zero)
                band_ref[which, 2 * h, 1, at, :] = jnp.where(low, zero, turned)
                band_ref[which, 2 * h + 1, 0, at, :] = jnp.where(low, turned, zero)
                band_ref[which, 2 * h + 1, 1, at, :] = jnp.where(low, zero, value)

    if edge_ref is not None:
        absent = jnp.where(first_ref[0] == 1, f32(-1e30), f32(0.0))
        bias = jnp.where(causal, f32(0.0), absent)
    for block in range(blocks):
        start = block * WINDOW
        band = pl.ds(start, 2 * WINDOW)
        for c in range(KVH):
            keys = jnp.concatenate([band_ref[0, c, 0, band, :], band_ref[0, c, 1, band, :]], axis=0)
            values = jnp.concatenate([band_ref[1, c, 0, band, :], band_ref[1, c, 1, band, :]], axis=0)
            q = jnp.concatenate(
                [q_ref[pl.ds(begin * WINDOW + start, WINDOW), c * 256 + p * LANES : c * 256 + (p + 1) * LANES] for p in range(2)],
                axis=0,
            )
            scores = lax.dot_general(q, keys, (((1,), (1,)), ((), ())), preferred_element_type=f32)
            lines = []
            totals = []
            for p in range(2):
                head = c * 4 + p * 2
                pieces = []
                sums = []
                tops = []
                for side in range(2):
                    base = side * 2 * WINDOW
                    s_prev = scores[p * WINDOW : (p + 1) * WINDOW, base : base + WINDOW]
                    s_cur = scores[p * WINDOW : (p + 1) * WINDOW, base + WINDOW : base + 2 * WINDOW]
                    s = jnp.where(causal, s_cur, s_prev)
                    if edge_ref is not None and block == 0:
                        s = s + bias
                    highest = jnp.maximum(jnp.max(s, axis=1, keepdims=True), sink_ref[head + side])
                    w = jnp.exp(s - highest)
                    sums.append(jnp.sum(w, axis=1, keepdims=True))
                    tops.append(highest)
                    rounded = w.astype(bf16)
                    pieces.append(jnp.where(causal, zero, rounded))
                    pieces.append(jnp.where(causal, rounded, zero))
                lines.append(jnp.concatenate(pieces, axis=1))
                sink = jnp.where(low, sink_ref[head], sink_ref[head + 1])
                rest = jnp.exp(sink - jnp.where(low, tops[0], tops[1]))
                totals.append(jnp.where(low, sums[0], sums[1]) + rest)
            summed = jnp.dot(jnp.concatenate(lines, axis=0), values, preferred_element_type=f32)
            for p in range(2):
                at = c * 256 + p * LANES
                done_ref[pl.ds(start, WINDOW), at : at + LANES] = (
                    summed[p * WINDOW : (p + 1) * WINDOW] / totals[p]
                ).astype(bf16)
    copy = pltpu.make_async_copy(
        done_ref, out_ref.at[begin * WINDOW : (begin + blocks) * WINDOW, :], copy_sem
    )
    copy.start()
    copy.wait()


def later_blocks_kernel(sink_ref, q_ref, kv_ref, out_ref, band_ref, done_ref, copy_sem):
    blocks = q_ref.shape[0] // WINDOW - 1
    attend_blocks(1, blocks, None, sink_ref, q_ref, kv_ref, None, out_ref, band_ref, done_ref, copy_sem)


def first_block_kernel(
    first_ref, sink_ref, q_ref, kv_ref, edge_ref, kept_ref, out_ref, band_ref, done_ref, copy_sem
):
    attend_blocks(0, 1, first_ref, sink_ref, q_ref, kv_ref, edge_ref, out_ref, band_ref, done_ref, copy_sem)


def passed_along(value):
    peers = lax.axis_size(("ep", "tp"))
    pairs = [(i, i + 1) for i in range(peers - 1)]
    return lax.ppermute(value, ("ep", "tp"), pairs)


def attend_window(queries, keys_values, sink_logits, edge):
    first = (lax.axis_index(("ep", "tp")) == 0).astype(jnp.int32).reshape(1)
    whole = pl.BlockSpec(memory_space=pltpu.VMEM)
    scalar = pl.BlockSpec(memory_space=pltpu.SMEM)
    outside = pl.BlockSpec(memory_space=pl.ANY)
    width = queries.shape[1]
    blocks = queries.shape[0] // WINDOW
    queries = near(queries)
    keys_values = near(keys_values)

    def scratch(count):
        return [
            pltpu.VMEM((2, KVH, 2, (count + 1) * WINDOW, LANES), jnp.bfloat16),
            pltpu.VMEM((count * WINDOW, width), jnp.bfloat16),
            pltpu.SemaphoreType.DMA,
        ]

    result = jax.ShapeDtypeStruct(queries.shape, jnp.bfloat16)
    later = pl.pallas_call(
        later_blocks_kernel,
        in_specs=[scalar, whole, whole],
        out_specs=outside,
        out_shape=result,
        scratch_shapes=scratch(blocks - 1),
        cost_estimate=pl.CostEstimate(flops=2 * 10**9, bytes_accessed=2 * 10**6, transcendentals=10**6),
        name="later_blocks",
    )(sink_logits, queries, keys_values)
    return pl.pallas_call(
        first_block_kernel,
        in_specs=[scalar, scalar, whole, whole, whole, outside],
        out_specs=outside,
        out_shape=result,
        scratch_shapes=scratch(1),
        input_output_aliases={5: 0},
        cost_estimate=pl.CostEstimate(flops=10**9, bytes_accessed=10**6, transcendentals=10**6),
        name="first_block",
    )(first, sink_logits, queries, keys_values, near(edge), later)


def dispatch_kernel(mine_ref, group_ref, member_ref, rows_ref, gain_ref, out_ref, place_ref, normed_ref, line_ref):
    f32 = jnp.float32
    bf16 = jnp.bfloat16
    tokens, width = rows_ref.shape
    pieces = width // LANES
    values = rows_ref[...].astype(f32)
    mean = jnp.mean(values * values, axis=1, keepdims=True)
    normed = (values * lax.rsqrt(mean + 1e-06) * gain_ref[...]).astype(bf16)
    normed_ref[...] = normed * bf16(ROW_SCALE)
    chosen = group_ref[...] * EPG + member_ref[...]
    which = lax.broadcasted_iota(jnp.int32, (EXPERTS, tokens), 0)
    first = (which == chosen[0:1, :]).astype(f32)
    second = (which == chosen[1:2, :]).astype(f32)
    before = (
        lax.broadcasted_iota(jnp.int32, (tokens, tokens), 0)
        < lax.broadcasted_iota(jnp.int32, (tokens, tokens), 1)
    ).astype(f32).astype(bf16)
    earlier = jnp.dot((first + second).astype(bf16), before, preferred_element_type=f32)
    places = []
    for k, hot in enumerate((first, second)):
        place = jnp.sum(hot * earlier, axis=0, keepdims=True).astype(jnp.int32)
        places.append(chosen[k : k + 1, :] * CAPACITY + place)
        place_ref[k : k + 1, :] = places[k]
    share = CAPACITY // TP
    slots = EXPERTS * share
    slot = lax.broadcasted_iota(jnp.int32, (slots, tokens), 0)
    wanted = (slot // share) * CAPACITY + mine_ref[0] * share + slot % share
    pick = ((places[0] == wanted) | (places[1] == wanted)).astype(f32).astype(bf16)
    picked = jnp.dot(pick, normed_ref[...], preferred_element_type=f32)
    for j in range(pieces):
        line_ref[pl.ds(j, slots, stride=pieces), :] = picked[:, j * LANES : (j + 1) * LANES]
    out_ref[...] = line_ref[...].reshape(out_ref.shape).astype(bf16)


def prepare_kernel(
    place_ref, weight_ref, gate_ref, up_ref, hot_ref, column_ref, both_ref, gate_sem, up_sem
):
    units = gate_ref.shape[1]
    gate_copy = pltpu.make_async_copy(gate_ref, both_ref.at[:, :units], gate_sem)
    up_copy = pltpu.make_async_copy(up_ref, both_ref.at[:, units:], up_sem)
    gate_copy.start()
    up_copy.start()
    f32 = jnp.float32
    bf16 = jnp.bfloat16
    tokens = place_ref.shape[1]
    slots = hot_ref.shape[2]
    for k in range(TOP):
        wide = jnp.broadcast_to(place_ref[k : k + 1, :].astype(f32), (LANES, tokens))
        place = wide.T.astype(jnp.int32)
        for j in range(slots // LANES):
            slot = lax.broadcasted_iota(jnp.int32, (tokens, LANES), 1) + j * LANES
            hot_ref[k, :, j * LANES : (j + 1) * LANES] = (place == slot).astype(f32).astype(bf16)
        column_ref[k] = jnp.broadcast_to(weight_ref[k : k + 1, :], (LANES, tokens)).T
    gate_copy.wait()
    up_copy.wait()


def hidden_kernel(y_ref, out_ref, plain_ref, ordered_ref):
    f32 = jnp.float32
    bf16 = jnp.bfloat16
    rows, width = plain_ref.shape
    share = CAPACITY // TP
    sources = rows // CAPACITY
    back = f32(1.0 / ROW_SCALE)
    peak = jnp.zeros((8, width), f32)
    step = share * sources
    for i in range(TP):
        gate = y_ref[i * step : (i + 1) * step, :width] * back
        up = y_ref[i * step : (i + 1) * step, width:] * back
        hidden = (gate / (1.0 + jnp.exp(-gate)) * up).astype(bf16).astype(f32)
        plain_ref[i * step : (i + 1) * step, :] = hidden
        peak = jnp.maximum(peak, jnp.max(jnp.abs(hidden).reshape(step // 8, 8, width), axis=0))
    top = jnp.max(jnp.max(peak, axis=1, keepdims=True), axis=0, keepdims=True)
    index = jnp.zeros((1, 1), f32)
    scale = jnp.full((1, 1), 2.0**71, f32)
    for i in range(1, LEVELS):
        reached = top >= f32(2.0 ** (8 * i - 64))
        index = jnp.where(reached, f32(i), index)
        scale = jnp.where(reached, f32(2.0 ** (71 - 8 * i)), scale)
    for i in range(TP):
        for j in range(share):
            part = plain_ref[pl.ds(i * step + j, sources, stride=share), :]
            ordered_ref[pl.ds(i * share + j, sources, stride=CAPACITY), :] = part
    out_ref[:rows, :] = (ordered_ref[...] * scale).astype(bf16)
    out_ref[rows:, :] = jnp.broadcast_to(index, (16, width)).astype(bf16)


def combine_kernel(hot_ref, column_ref, rows_ref, out_ref):
    total = None
    for k in range(TOP):
        picked = jnp.dot(hot_ref[k], rows_ref[...], preferred_element_type=jnp.float32)
        part = column_ref[k] * picked
        total = part if total is None else total + part
    out_ref[...] = total.astype(jnp.bfloat16)


def route_experts(
    moe_rows, norm_gain, group_choice, member_choice, route_weight, w_gate, w_up, w_down, last_rows
):
    bf16 = jnp.bfloat16
    tokens, width = moe_rows.shape
    share = CAPACITY // TP
    slots = EXPERTS * share
    mine = lax.axis_index("tp").astype(jnp.int32).reshape(1)
    whole = pl.BlockSpec(memory_space=pltpu.VMEM)
    scalar = pl.BlockSpec(memory_space=pltpu.SMEM)
    outside = pl.BlockSpec(memory_space=pl.ANY)
    outgoing, places = pl.pallas_call(
        dispatch_kernel,
        in_specs=[scalar, whole, whole, whole, whole],
        out_specs=[whole, whole],
        out_shape=[
            jax.ShapeDtypeStruct((EXPERTS, share * width // LANES, LANES), bf16),
            pltpu.VMEM((TOP, tokens), jnp.int32),
        ],
        scratch_shapes=[
            pltpu.VMEM((tokens, width), bf16),
            pltpu.VMEM((slots * width // LANES, LANES), jnp.float32),
        ],
        name="dispatch",
    )(mine, group_choice[None, :], member_choice.T, moe_rows, norm_gain[None, :])
    incoming = lax.all_to_all(outgoing, "ep", 0, 0, tiled=True)
    hots, columns, both = pl.pallas_call(
        prepare_kernel,
        in_specs=[whole, whole, outside, outside],
        out_specs=[whole, whole, whole],
        out_shape=[
            pltpu.VMEM((TOP, tokens, EXPERTS * CAPACITY), bf16),
            pltpu.VMEM((TOP, tokens, LANES), jnp.float32),
            pltpu.VMEM((width, 2 * w_gate.shape[2]), bf16),
        ],
        scratch_shapes=[pltpu.SemaphoreType.DMA, pltpu.SemaphoreType.DMA],
        name="prepare",
    )(near(places), route_weight.T, w_gate[0], w_up[0])
    incoming, last_rows, hots, columns, both = lax.optimization_barrier(
        (incoming, last_rows, hots, columns, both)
    )
    shared = incoming.reshape(slots, width).astype(jnp.float16)
    block_rows = lax.all_gather(shared, "tp", axis=0, tiled=True).astype(bf16)
    total = block_rows.shape[0]
    y = jnp.dot(block_rows, both, preferred_element_type=jnp.float32)
    units = w_gate.shape[2]
    hidden = pl.pallas_call(
        hidden_kernel,
        in_specs=[whole],
        out_specs=whole,
        out_shape=pltpu.VMEM((total + 16, units), bf16),
        scratch_shapes=[pltpu.VMEM((total, units), jnp.float32)] * 2,
        name="hidden",
    )(near(y))
    spread = lax.all_gather(hidden.astype(jnp.float16), "tp", axis=0, tiled=False)
    index = spread[:, total, 0].astype(jnp.float32)
    factor = jnp.full(index.shape, 2.0**-71, jnp.float32)
    for i in range(1, LEVELS):
        factor = jnp.where(index == i, 2.0 ** (8 * i - 71), factor)
    out_width = w_down.shape[2]
    weight = w_down[0].reshape(TP, units, out_width).astype(jnp.float32) * factor[:, None, None]
    produced = jnp.einsum(
        "trk,tko->ro",
        spread[:, :total].astype(bf16),
        weight.astype(bf16),
        preferred_element_type=jnp.float32,
    ).astype(bf16)
    returned = lax.all_to_all(
        produced.reshape(total // CAPACITY, CAPACITY, out_width), "ep", 0, 0, tiled=True
    )
    mixed = pl.pallas_call(
        combine_kernel,
        in_specs=[whole, whole, whole],
        out_specs=whole,
        out_shape=jax.ShapeDtypeStruct((tokens, out_width), bf16),
        name="combine",
    )(near(hots), near(columns), near(returned.reshape(EXPERTS * CAPACITY, out_width)))
    return mixed, last_rows, produced


def shards(
    queries,
    keys_values,
    sink_logits,
    moe_rows,
    norm_gain,
    group_choice,
    member_choice,
    route_weight,
    w_gate,
    w_up,
    w_down,
):
    last_rows = keys_values[:, keys_values.shape[1] - WINDOW :, :]
    mixed, last_rows, produced = route_experts(
        moe_rows,
        norm_gain,
        group_choice,
        member_choice,
        route_weight,
        w_gate,
        w_up,
        w_down,
        last_rows,
    )
    last_rows, sink_logits, produced = lax.optimization_barrier((last_rows, sink_logits, produced))
    edge = passed_along(last_rows)
    attended = attend_window(queries, keys_values, sink_logits, edge)
    return (attended, mixed)


def solution(mesh):
    in_specs = (
        P(("ep", "tp"), None),
        P(None, ("ep", "tp"), None),
        P(),
        P("ep", None),
        P(),
        P("ep"),
        P("ep", None),
        P("ep", None),
        P("ep", None, "tp"),
        P("ep", None, "tp"),
        P("ep", None, "tp"),
    )
    out_specs = (P(("ep", "tp"), None), P("ep", "tp"))
    return jax.shard_map(shards, mesh=mesh, in_specs=in_specs, out_specs=out_specs, check_vma=False)
```

```python
import jax
import jax.numpy as jnp
from jax import lax
from jax.experimental import pallas as pl
from jax.experimental.pallas import tpu as pltpu
from jax.sharding import PartitionSpec as P


KVH = 4
HD = 64
WINDOW = 128
EPG = 4
TOP = 2
LANES = 128
EXPERTS = 32
CAPACITY = 32
TP = 16
ROW_SCALE = 256.0
LEVELS = 11


def near(value):
    return pltpu.with_memory_space_constraint(value, pltpu.VMEM)


def attend_blocks(
    begin, blocks, first_ref, sink_ref, q_ref, kv_ref, edge_ref, out_ref, band_ref, done_ref, copy_sem
):
    f32 = jnp.float32
    bf16 = jnp.bfloat16
    row = lax.broadcasted_iota(jnp.int32, (WINDOW, WINDOW), 0)
    col = lax.broadcasted_iota(jnp.int32, (WINDOW, WINDOW), 1)
    causal = col <= row
    low = lax.broadcasted_iota(jnp.int32, (WINDOW, LANES), 1) < HD
    zero = jnp.zeros((WINDOW, LANES), bf16)
    for which in range(2):
        for part in range(blocks + 1):
            for h in range(KVH // 2):
                lanes = slice(h * LANES, (h + 1) * LANES)
                if part == 0 and edge_ref is not None:
                    value = edge_ref[which, :, lanes]
                else:
                    at = begin + part - 1
                    value = kv_ref[which, at * WINDOW : (at + 1) * WINDOW, lanes]
                if which == 0:
                    value = value * bf16(HD ** (-0.5))
                turned = pltpu.roll(value.astype(f32), HD, 1).astype(bf16)
                at = slice(part * WINDOW, (part + 1) * WINDOW)
                band_ref[which, 2 * h, 0, at, :] = jnp.where(low, value, zero)
                band_ref[which, 2 * h, 1, at, :] = jnp.where(low, zero, turned)
                band_ref[which, 2 * h + 1, 0, at, :] = jnp.where(low, turned, zero)
                band_ref[which, 2 * h + 1, 1, at, :] = jnp.where(low, zero, value)

    def written(block, c):
        lanes = pl.ds(c * 256, 256)
        return pltpu.make_async_copy(
            done_ref.at[pl.ds(block * WINDOW, WINDOW), lanes],
            out_ref.at[pl.ds((begin + block) * WINDOW, WINDOW), lanes],
            copy_sem.at[block, c],
        )

    if edge_ref is not None:
        absent = jnp.where(first_ref[0] == 1, f32(-1e30), f32(0.0))
        bias = jnp.where(causal, f32(0.0), absent)
    for block in range(blocks):
        start = block * WINDOW
        band = pl.ds(start, 2 * WINDOW)
        for c in range(KVH):
            keys = jnp.concatenate([band_ref[0, c, 0, band, :], band_ref[0, c, 1, band, :]], axis=0)
            values = jnp.concatenate([band_ref[1, c, 0, band, :], band_ref[1, c, 1, band, :]], axis=0)
            q = jnp.concatenate(
                [q_ref[pl.ds(begin * WINDOW + start, WINDOW), c * 256 + p * LANES : c * 256 + (p + 1) * LANES] for p in range(2)],
                axis=0,
            )
            scores = lax.dot_general(q, keys, (((1,), (1,)), ((), ())), preferred_element_type=f32)
            lines = []
            totals = []
            for p in range(2):
                head = c * 4 + p * 2
                pieces = []
                sums = []
                tops = []
                for side in range(2):
                    base = side * 2 * WINDOW
                    s_prev = scores[p * WINDOW : (p + 1) * WINDOW, base : base + WINDOW]
                    s_cur = scores[p * WINDOW : (p + 1) * WINDOW, base + WINDOW : base + 2 * WINDOW]
                    s = jnp.where(causal, s_cur, s_prev)
                    if edge_ref is not None and block == 0:
                        s = s + bias
                    highest = jnp.maximum(jnp.max(s, axis=1, keepdims=True), sink_ref[head + side])
                    w = jnp.exp(s - highest)
                    sums.append(jnp.sum(w, axis=1, keepdims=True))
                    tops.append(highest)
                    rounded = w.astype(bf16)
                    pieces.append(jnp.where(causal, zero, rounded))
                    pieces.append(jnp.where(causal, rounded, zero))
                lines.append(jnp.concatenate(pieces, axis=1))
                sink = jnp.where(low, sink_ref[head], sink_ref[head + 1])
                rest = jnp.exp(sink - jnp.where(low, tops[0], tops[1]))
                totals.append(jnp.where(low, sums[0], sums[1]) + rest)
            summed = jnp.dot(jnp.concatenate(lines, axis=0), values, preferred_element_type=f32)
            for p in range(2):
                at = c * 256 + p * LANES
                done_ref[pl.ds(start, WINDOW), at : at + LANES] = (
                    summed[p * WINDOW : (p + 1) * WINDOW] / totals[p]
                ).astype(bf16)
            written(block, c).start()
    for block in range(blocks):
        for c in range(KVH):
            written(block, c).wait()


def later_blocks_kernel(sink_ref, q_ref, kv_ref, out_ref, band_ref, done_ref, copy_sem):
    blocks = q_ref.shape[0] // WINDOW - 1
    attend_blocks(1, blocks, None, sink_ref, q_ref, kv_ref, None, out_ref, band_ref, done_ref, copy_sem)


def first_block_kernel(
    first_ref, sink_ref, q_ref, kv_ref, edge_ref, kept_ref, out_ref, band_ref, done_ref, copy_sem
):
    attend_blocks(0, 1, first_ref, sink_ref, q_ref, kv_ref, edge_ref, out_ref, band_ref, done_ref, copy_sem)


def passed_along(value):
    peers = lax.axis_size(("ep", "tp"))
    pairs = [(i, i + 1) for i in range(peers - 1)]
    return lax.ppermute(value, ("ep", "tp"), pairs)


def attend_window(queries, keys_values, sink_logits, edge):
    first = (lax.axis_index(("ep", "tp")) == 0).astype(jnp.int32).reshape(1)
    whole = pl.BlockSpec(memory_space=pltpu.VMEM)
    scalar = pl.BlockSpec(memory_space=pltpu.SMEM)
    outside = pl.BlockSpec(memory_space=pl.ANY)
    width = queries.shape[1]
    blocks = queries.shape[0] // WINDOW
    queries = near(queries)
    keys_values = near(keys_values)

    def scratch(count):
        return [
            pltpu.VMEM((2, KVH, 2, (count + 1) * WINDOW, LANES), jnp.bfloat16),
            pltpu.VMEM((count * WINDOW, width), jnp.bfloat16),
            pltpu.SemaphoreType.DMA((count, KVH)),
        ]

    result = jax.ShapeDtypeStruct(queries.shape, jnp.bfloat16)
    later = pl.pallas_call(
        later_blocks_kernel,
        in_specs=[scalar, whole, whole],
        out_specs=outside,
        out_shape=result,
        scratch_shapes=scratch(blocks - 1),
        cost_estimate=pl.CostEstimate(flops=2 * 10**9, bytes_accessed=2 * 10**6, transcendentals=10**6),
        name="later_blocks",
    )(sink_logits, queries, keys_values)
    return pl.pallas_call(
        first_block_kernel,
        in_specs=[scalar, scalar, whole, whole, whole, outside],
        out_specs=outside,
        out_shape=result,
        scratch_shapes=scratch(1),
        input_output_aliases={5: 0},
        cost_estimate=pl.CostEstimate(flops=10**9, bytes_accessed=10**6, transcendentals=10**6),
        name="first_block",
    )(first, sink_logits, queries, keys_values, near(edge), later)


def dispatch_kernel(
    mine_ref,
    far_group_ref,
    far_member_ref,
    far_rows_ref,
    far_gain_ref,
    out_ref,
    place_ref,
    group_ref,
    member_ref,
    rows_ref,
    gain_ref,
    line_ref,
    ready_ref,
    sems,
):
    f32 = jnp.float32
    bf16 = jnp.bfloat16
    tokens, width = rows_ref.shape
    rows_copy = pltpu.make_async_copy(far_rows_ref, rows_ref, sems.at[0])
    group_copy = pltpu.make_async_copy(far_group_ref, group_ref, sems.at[1])
    member_copy = pltpu.make_async_copy(far_member_ref, member_ref, sems.at[2])
    gain_copy = pltpu.make_async_copy(far_gain_ref, gain_ref, sems.at[3])
    group_copy.start()
    member_copy.start()
    rows_copy.start()
    gain_copy.start()
    which = lax.broadcasted_iota(jnp.int32, (EXPERTS, tokens), 0)
    before = (
        lax.broadcasted_iota(jnp.int32, (tokens, tokens), 0)
        < lax.broadcasted_iota(jnp.int32, (tokens, tokens), 1)
    ).astype(f32).astype(bf16)
    group_copy.wait()
    member_copy.wait()
    chosen = group_ref[...] * EPG + member_ref[...]
    first = (which == chosen[0:1, :]).astype(f32)
    second = (which == chosen[1:2, :]).astype(f32)
    earlier = jnp.dot((first + second).astype(bf16), before, preferred_element_type=f32)
    places = []
    for k, hot in enumerate((first, second)):
        place = jnp.sum(hot * earlier, axis=0, keepdims=True).astype(jnp.int32)
        places.append(chosen[k : k + 1, :] * CAPACITY + place)
        place_ref[k : k + 1, :] = places[k]
    share = CAPACITY // TP
    slots = EXPERTS * share
    slot = lax.broadcasted_iota(jnp.int32, (slots, tokens), 0)
    wanted = (slot // share) * CAPACITY + mine_ref[0] * share + slot % share
    pick = ((places[0] == wanted) | (places[1] == wanted)).astype(f32).astype(bf16)
    rows_copy.wait()
    gain_copy.wait()
    values = jnp.dot(pick, rows_ref[...], preferred_element_type=f32)
    mean = jnp.mean(values * values, axis=1, keepdims=True)
    normed = (values * lax.rsqrt(mean + 1e-06) * gain_ref[...]).astype(bf16).astype(f32) * ROW_SCALE
    pieces = width // LANES
    for j in range(pieces):
        line_ref[pl.ds(j, slots, stride=pieces), :] = normed[:, j * LANES : (j + 1) * LANES]
    half = EXPERTS // 2
    rows = share * pieces
    copies = []
    for i in range(2):
        part = line_ref[i * half * rows : (i + 1) * half * rows, :].reshape(half, rows, LANES)
        ready_ref[i * half : (i + 1) * half] = part.astype(bf16)
        copies.append(
            pltpu.make_async_copy(
                ready_ref.at[pl.ds(i * half, half)], out_ref.at[pl.ds(i * half, half)], sems.at[4 + i]
            )
        )
        copies[i].start()
    for copy in copies:
        copy.wait()


def prepare_kernel(
    place_ref, weight_ref, gate_ref, up_ref, hot_ref, column_ref, both_ref, gate_sem, up_sem
):
    units = gate_ref.shape[1]
    gate_copy = pltpu.make_async_copy(gate_ref, both_ref.at[:, :units], gate_sem)
    up_copy = pltpu.make_async_copy(up_ref, both_ref.at[:, units:], up_sem)
    gate_copy.start()
    up_copy.start()
    f32 = jnp.float32
    bf16 = jnp.bfloat16
    tokens = place_ref.shape[1]
    slots = hot_ref.shape[2]
    for k in range(TOP):
        wide = jnp.broadcast_to(place_ref[k : k + 1, :].astype(f32), (LANES, tokens))
        place = wide.T.astype(jnp.int32)
        for j in range(slots // LANES):
            slot = lax.broadcasted_iota(jnp.int32, (tokens, LANES), 1) + j * LANES
            hot_ref[k, :, j * LANES : (j + 1) * LANES] = (place == slot).astype(f32).astype(bf16)
        column_ref[k] = jnp.broadcast_to(weight_ref[k : k + 1, :], (LANES, tokens)).T
    gate_copy.wait()
    up_copy.wait()


def hidden_kernel(y_ref, out_ref, plain_ref, ordered_ref):
    f32 = jnp.float32
    bf16 = jnp.bfloat16
    rows, width = plain_ref.shape
    share = CAPACITY // TP
    sources = rows // CAPACITY
    back = f32(1.0 / ROW_SCALE)
    peak = jnp.zeros((8, width), f32)
    step = share * sources
    for i in range(TP):
        gate = y_ref[i * step : (i + 1) * step, :width] * back
        up = y_ref[i * step : (i + 1) * step, width:] * back
        hidden = (gate / (1.0 + jnp.exp(-gate)) * up).astype(bf16).astype(f32)
        plain_ref[i * step : (i + 1) * step, :] = hidden
        peak = jnp.maximum(peak, jnp.max(jnp.abs(hidden).reshape(step // 8, 8, width), axis=0))
    top = jnp.max(jnp.max(peak, axis=1, keepdims=True), axis=0, keepdims=True)
    index = jnp.zeros((1, 1), f32)
    scale = jnp.full((1, 1), 2.0**71, f32)
    for i in range(1, LEVELS):
        reached = top >= f32(2.0 ** (8 * i - 64))
        index = jnp.where(reached, f32(i), index)
        scale = jnp.where(reached, f32(2.0 ** (71 - 8 * i)), scale)
    for i in range(TP):
        for j in range(share):
            part = plain_ref[pl.ds(i * step + j, sources, stride=share), :]
            ordered_ref[pl.ds(i * share + j, sources, stride=CAPACITY), :] = part
    out_ref[:rows, :] = (ordered_ref[...] * scale).astype(bf16)
    out_ref[rows:, :] = jnp.broadcast_to(index, (16, width)).astype(bf16)


def combine_kernel(hot_ref, column_ref, rows_ref, out_ref):
    total = None
    for k in range(TOP):
        picked = jnp.dot(hot_ref[k], rows_ref[...], preferred_element_type=jnp.float32)
        part = column_ref[k] * picked
        total = part if total is None else total + part
    out_ref[...] = total.astype(jnp.bfloat16)


def route_experts(
    moe_rows, norm_gain, group_choice, member_choice, route_weight, w_gate, w_up, w_down, last_rows
):
    bf16 = jnp.bfloat16
    tokens, width = moe_rows.shape
    share = CAPACITY // TP
    slots = EXPERTS * share
    mine = lax.axis_index("tp").astype(jnp.int32).reshape(1)
    whole = pl.BlockSpec(memory_space=pltpu.VMEM)
    scalar = pl.BlockSpec(memory_space=pltpu.SMEM)
    outside = pl.BlockSpec(memory_space=pl.ANY)
    outgoing, places = pl.pallas_call(
        dispatch_kernel,
        in_specs=[scalar, outside, outside, outside, outside],
        out_specs=[outside, whole],
        out_shape=[
            jax.ShapeDtypeStruct((EXPERTS, share * width // LANES, LANES), bf16),
            pltpu.VMEM((TOP, tokens), jnp.int32),
        ],
        scratch_shapes=[
            pltpu.VMEM((1, tokens), jnp.int32),
            pltpu.VMEM((TOP, tokens), jnp.int32),
            pltpu.VMEM((tokens, width), bf16),
            pltpu.VMEM((1, width), jnp.float32),
            pltpu.VMEM((slots * width // LANES, LANES), jnp.float32),
            pltpu.VMEM((EXPERTS, share * width // LANES, LANES), bf16),
            pltpu.SemaphoreType.DMA((6,)),
        ],
        name="dispatch",
    )(mine, group_choice[None, :], member_choice.T, moe_rows, norm_gain[None, :])
    incoming = lax.all_to_all(outgoing, "ep", 0, 0, tiled=True)
    hots, columns, both = pl.pallas_call(
        prepare_kernel,
        in_specs=[whole, whole, outside, outside],
        out_specs=[whole, whole, whole],
        out_shape=[
            pltpu.VMEM((TOP, tokens, EXPERTS * CAPACITY), bf16),
            pltpu.VMEM((TOP, tokens, LANES), jnp.float32),
            pltpu.VMEM((width, 2 * w_gate.shape[2]), bf16),
        ],
        scratch_shapes=[pltpu.SemaphoreType.DMA, pltpu.SemaphoreType.DMA],
        name="prepare",
    )(near(places), route_weight.T, w_gate[0], w_up[0])
    incoming, last_rows, hots, columns, both = lax.optimization_barrier(
        (incoming, last_rows, hots, columns, both)
    )
    shared = incoming.reshape(slots, width).astype(jnp.float16)
    block_rows = lax.all_gather(shared, "tp", axis=0, tiled=True).astype(bf16)
    total = block_rows.shape[0]
    y = jnp.dot(block_rows, both, preferred_element_type=jnp.float32)
    units = w_gate.shape[2]
    hidden = pl.pallas_call(
        hidden_kernel,
        in_specs=[whole],
        out_specs=whole,
        out_shape=pltpu.VMEM((total + 16, units), bf16),
        scratch_shapes=[pltpu.VMEM((total, units), jnp.float32)] * 2,
        name="hidden",
    )(near(y))
    spread = lax.all_gather(hidden.astype(jnp.float16), "tp", axis=0, tiled=False)
    index = spread[:, total, 0].astype(jnp.float32)
    factor = jnp.full(index.shape, 2.0**-71, jnp.float32)
    for i in range(1, LEVELS):
        factor = jnp.where(index == i, 2.0 ** (8 * i - 71), factor)
    out_width = w_down.shape[2]
    weight = w_down[0].reshape(TP, units, out_width).astype(jnp.float32) * factor[:, None, None]
    produced = jnp.einsum(
        "trk,tko->ro",
        spread[:, :total].astype(bf16),
        weight.astype(bf16),
        preferred_element_type=jnp.float32,
    ).astype(bf16)
    returned = lax.all_to_all(
        produced.reshape(total // CAPACITY, CAPACITY, out_width), "ep", 0, 0, tiled=True
    )
    mixed = pl.pallas_call(
        combine_kernel,
        in_specs=[whole, whole, whole],
        out_specs=whole,
        out_shape=jax.ShapeDtypeStruct((tokens, out_width), bf16),
        name="combine",
    )(near(hots), near(columns), near(returned.reshape(EXPERTS * CAPACITY, out_width)))
    return mixed, last_rows, produced


def shards(
    queries,
    keys_values,
    sink_logits,
    moe_rows,
    norm_gain,
    group_choice,
    member_choice,
    route_weight,
    w_gate,
    w_up,
    w_down,
):
    last_rows = keys_values[:, keys_values.shape[1] - WINDOW :, :]
    mixed, last_rows, produced = route_experts(
        moe_rows,
        norm_gain,
        group_choice,
        member_choice,
        route_weight,
        w_gate,
        w_up,
        w_down,
        last_rows,
    )
    last_rows, sink_logits, produced = lax.optimization_barrier((last_rows, sink_logits, produced))
    edge = passed_along(last_rows)
    attended = attend_window(queries, keys_values, sink_logits, edge)
    return (attended, mixed)


def solution(mesh):
    in_specs = (
        P(("ep", "tp"), None),
        P(None, ("ep", "tp"), None),
        P(),
        P("ep", None),
        P(),
        P("ep"),
        P("ep", None),
        P("ep", None),
        P("ep", None, "tp"),
        P("ep", None, "tp"),
        P("ep", None, "tp"),
    )
    out_specs = (P(("ep", "tp"), None), P("ep", "tp"))
    return jax.shard_map(shards, mesh=mesh, in_specs=in_specs, out_specs=out_specs, check_vma=False)
```

```python
import jax
import jax.numpy as jnp
from jax import lax
from jax.experimental import pallas as pl
from jax.experimental.pallas import tpu as pltpu
from jax.sharding import PartitionSpec as P


KVH = 4
HD = 64
WINDOW = 128
EPG = 4
TOP = 2
LANES = 128
EXPERTS = 32
CAPACITY = 32
TP = 16
ROW_SCALE = 256.0
LEVELS = 11


def near(value):
    return pltpu.with_memory_space_constraint(value, pltpu.VMEM)


def attend_blocks(
    begin, blocks, first_ref, sink_ref, q_ref, kv_ref, edge_ref, shared_ref, out_ref, band_ref, done_ref, copy_sem
):
    f32 = jnp.float32
    bf16 = jnp.bfloat16
    row = lax.broadcasted_iota(jnp.int32, (WINDOW, WINDOW), 0)
    col = lax.broadcasted_iota(jnp.int32, (WINDOW, WINDOW), 1)
    causal = col <= row
    low = lax.broadcasted_iota(jnp.int32, (WINDOW, LANES), 1) < HD
    zero = jnp.zeros((WINDOW, LANES), bf16)
    parts = blocks + 1
    if edge_ref is not None:
        parts = 1
        band_ref[:, :, :, WINDOW : 2 * WINDOW, :] = shared_ref[...]
    for which in range(2):
        for part in range(parts):
            for h in range(KVH // 2):
                lanes = slice(h * LANES, (h + 1) * LANES)
                if part == 0 and edge_ref is not None:
                    value = edge_ref[which, :, lanes]
                else:
                    at = begin + part - 1
                    value = kv_ref[which, at * WINDOW : (at + 1) * WINDOW, lanes]
                if which == 0:
                    value = value * bf16(HD ** (-0.5))
                turned = pltpu.roll(value.astype(f32), HD, 1).astype(bf16)
                at = slice(part * WINDOW, (part + 1) * WINDOW)
                band_ref[which, 2 * h, 0, at, :] = jnp.where(low, value, zero)
                band_ref[which, 2 * h, 1, at, :] = jnp.where(low, zero, turned)
                band_ref[which, 2 * h + 1, 0, at, :] = jnp.where(low, turned, zero)
                band_ref[which, 2 * h + 1, 1, at, :] = jnp.where(low, zero, value)

    if edge_ref is None:
        shared_ref[...] = band_ref[:, :, :, :WINDOW, :]

    def written(block, c):
        lanes = pl.ds(c * 256, 256)
        return pltpu.make_async_copy(
            done_ref.at[pl.ds(block * WINDOW, WINDOW), lanes],
            out_ref.at[pl.ds((begin + block) * WINDOW, WINDOW), lanes],
            copy_sem.at[block, c],
        )

    if edge_ref is not None:
        absent = jnp.where(first_ref[0] == 1, f32(-1e30), f32(0.0))
        bias = jnp.where(causal, f32(0.0), absent)
    for block in range(blocks):
        start = block * WINDOW
        band = pl.ds(start, 2 * WINDOW)
        for c in range(KVH):
            keys = jnp.concatenate([band_ref[0, c, 0, band, :], band_ref[0, c, 1, band, :]], axis=0)
            values = jnp.concatenate([band_ref[1, c, 0, band, :], band_ref[1, c, 1, band, :]], axis=0)
            q = jnp.concatenate(
                [q_ref[pl.ds(begin * WINDOW + start, WINDOW), c * 256 + p * LANES : c * 256 + (p + 1) * LANES] for p in range(2)],
                axis=0,
            )
            scores = lax.dot_general(q, keys, (((1,), (1,)), ((), ())), preferred_element_type=f32)
            lines = []
            totals = []
            for p in range(2):
                head = c * 4 + p * 2
                pieces = []
                sums = []
                tops = []
                for side in range(2):
                    base = side * 2 * WINDOW
                    s_prev = scores[p * WINDOW : (p + 1) * WINDOW, base : base + WINDOW]
                    s_cur = scores[p * WINDOW : (p + 1) * WINDOW, base + WINDOW : base + 2 * WINDOW]
                    s = jnp.where(causal, s_cur, s_prev)
                    if edge_ref is not None and block == 0:
                        s = s + bias
                    highest = jnp.maximum(jnp.max(s, axis=1, keepdims=True), sink_ref[head + side])
                    w = jnp.exp(s - highest)
                    sums.append(jnp.sum(w, axis=1, keepdims=True))
                    tops.append(highest)
                    rounded = w.astype(bf16)
                    pieces.append(jnp.where(causal, zero, rounded))
                    pieces.append(jnp.where(causal, rounded, zero))
                lines.append(jnp.concatenate(pieces, axis=1))
                sink = jnp.where(low, sink_ref[head], sink_ref[head + 1])
                rest = jnp.exp(sink - jnp.where(low, tops[0], tops[1]))
                totals.append(jnp.where(low, sums[0], sums[1]) + rest)
            summed = jnp.dot(jnp.concatenate(lines, axis=0), values, preferred_element_type=f32)
            for p in range(2):
                at = c * 256 + p * LANES
                done_ref[pl.ds(start, WINDOW), at : at + LANES] = (
                    summed[p * WINDOW : (p + 1) * WINDOW] / totals[p]
                ).astype(bf16)
            written(block, c).start()
    for block in range(blocks):
        for c in range(KVH):
            written(block, c).wait()


def later_blocks_kernel(sink_ref, q_ref, kv_ref, out_ref, shared_ref, band_ref, done_ref, copy_sem):
    blocks = q_ref.shape[0] // WINDOW - 1
    attend_blocks(
        1, blocks, None, sink_ref, q_ref, kv_ref, None, shared_ref, out_ref, band_ref, done_ref, copy_sem
    )


def first_block_kernel(
    first_ref, sink_ref, q_ref, shared_ref, edge_ref, kept_ref, out_ref, band_ref, done_ref, copy_sem
):
    attend_blocks(
        0, 1, first_ref, sink_ref, q_ref, None, edge_ref, shared_ref, out_ref, band_ref, done_ref, copy_sem
    )


def passed_along(value):
    peers = lax.axis_size(("ep", "tp"))
    pairs = [(i, i + 1) for i in range(peers - 1)]
    return lax.ppermute(value, ("ep", "tp"), pairs)


def attend_window(queries, keys_values, sink_logits, edge):
    first = (lax.axis_index(("ep", "tp")) == 0).astype(jnp.int32).reshape(1)
    whole = pl.BlockSpec(memory_space=pltpu.VMEM)
    scalar = pl.BlockSpec(memory_space=pltpu.SMEM)
    outside = pl.BlockSpec(memory_space=pl.ANY)
    width = queries.shape[1]
    blocks = queries.shape[0] // WINDOW
    queries = near(queries)
    keys_values = near(keys_values)

    def scratch(count):
        return [
            pltpu.VMEM((2, KVH, 2, (count + 1) * WINDOW, LANES), jnp.bfloat16),
            pltpu.VMEM((count * WINDOW, width), jnp.bfloat16),
            pltpu.SemaphoreType.DMA((count, KVH)),
        ]

    result = jax.ShapeDtypeStruct(queries.shape, jnp.bfloat16)
    later, shared = pl.pallas_call(
        later_blocks_kernel,
        in_specs=[scalar, whole, whole],
        out_specs=[outside, whole],
        out_shape=[result, pltpu.VMEM((2, KVH, 2, WINDOW, LANES), jnp.bfloat16)],
        scratch_shapes=scratch(blocks - 1),
        cost_estimate=pl.CostEstimate(flops=2 * 10**9, bytes_accessed=2 * 10**6, transcendentals=10**6),
        name="later_blocks",
    )(sink_logits, queries, keys_values)
    return pl.pallas_call(
        first_block_kernel,
        in_specs=[scalar, scalar, whole, whole, whole, outside],
        out_specs=outside,
        out_shape=result,
        scratch_shapes=scratch(1),
        input_output_aliases={5: 0},
        cost_estimate=pl.CostEstimate(flops=10**9, bytes_accessed=10**6, transcendentals=10**6),
        name="first_block",
    )(first, sink_logits, queries, near(shared), near(edge), later)


def dispatch_kernel(
    mine_ref,
    far_group_ref,
    far_member_ref,
    far_rows_ref,
    far_gain_ref,
    out_ref,
    place_ref,
    group_ref,
    member_ref,
    rows_ref,
    gain_ref,
    line_ref,
    ready_ref,
    sems,
):
    f32 = jnp.float32
    bf16 = jnp.bfloat16
    tokens, width = rows_ref.shape
    rows_copy = pltpu.make_async_copy(far_rows_ref, rows_ref, sems.at[0])
    group_copy = pltpu.make_async_copy(far_group_ref, group_ref, sems.at[1])
    member_copy = pltpu.make_async_copy(far_member_ref, member_ref, sems.at[2])
    gain_copy = pltpu.make_async_copy(far_gain_ref, gain_ref, sems.at[3])
    group_copy.start()
    member_copy.start()
    rows_copy.start()
    gain_copy.start()
    which = lax.broadcasted_iota(jnp.int32, (EXPERTS, tokens), 0)
    before = (
        lax.broadcasted_iota(jnp.int32, (tokens, tokens), 0)
        < lax.broadcasted_iota(jnp.int32, (tokens, tokens), 1)
    ).astype(f32).astype(bf16)
    group_copy.wait()
    member_copy.wait()
    chosen = group_ref[...] * EPG + member_ref[...]
    first = (which == chosen[0:1, :]).astype(f32)
    second = (which == chosen[1:2, :]).astype(f32)
    earlier = jnp.dot((first + second).astype(bf16), before, preferred_element_type=f32)
    places = []
    for k, hot in enumerate((first, second)):
        place = jnp.sum(hot * earlier, axis=0, keepdims=True).astype(jnp.int32)
        places.append(chosen[k : k + 1, :] * CAPACITY + place)
        place_ref[k : k + 1, :] = places[k]
    share = CAPACITY // TP
    slots = EXPERTS * share
    slot = lax.broadcasted_iota(jnp.int32, (slots, tokens), 0)
    wanted = (slot // share) * CAPACITY + mine_ref[0] * share + slot % share
    pick = ((places[0] == wanted) | (places[1] == wanted)).astype(f32).astype(bf16)
    rows_copy.wait()
    gain_copy.wait()
    values = jnp.dot(pick, rows_ref[...], preferred_element_type=f32)
    mean = jnp.mean(values * values, axis=1, keepdims=True)
    normed = (values * lax.rsqrt(mean + 1e-06) * gain_ref[...]).astype(bf16).astype(f32) * ROW_SCALE
    pieces = width // LANES
    for j in range(pieces):
        line_ref[pl.ds(j, slots, stride=pieces), :] = normed[:, j * LANES : (j + 1) * LANES]
    half = EXPERTS // 2
    rows = share * pieces
    copies = []
    for i in range(2):
        part = line_ref[i * half * rows : (i + 1) * half * rows, :].reshape(half, rows, LANES)
        ready_ref[i * half : (i + 1) * half] = part.astype(bf16)
        copies.append(
            pltpu.make_async_copy(
                ready_ref.at[pl.ds(i * half, half)], out_ref.at[pl.ds(i * half, half)], sems.at[4 + i]
            )
        )
        copies[i].start()
    for copy in copies:
        copy.wait()


def prepare_kernel(
    place_ref, weight_ref, gate_ref, up_ref, hot_ref, column_ref, both_ref, gate_sem, up_sem
):
    units = gate_ref.shape[1]
    gate_copy = pltpu.make_async_copy(gate_ref, both_ref.at[:, :units], gate_sem)
    up_copy = pltpu.make_async_copy(up_ref, both_ref.at[:, units:], up_sem)
    gate_copy.start()
    up_copy.start()
    f32 = jnp.float32
    bf16 = jnp.bfloat16
    tokens = place_ref.shape[1]
    slots = hot_ref.shape[2]
    for k in range(TOP):
        wide = jnp.broadcast_to(place_ref[k : k + 1, :].astype(f32), (LANES, tokens))
        place = wide.T.astype(jnp.int32)
        for j in range(slots // LANES):
            slot = lax.broadcasted_iota(jnp.int32, (tokens, LANES), 1) + j * LANES
            hot_ref[k, :, j * LANES : (j + 1) * LANES] = (place == slot).astype(f32).astype(bf16)
        column_ref[k] = jnp.broadcast_to(weight_ref[k : k + 1, :], (LANES, tokens)).T
    gate_copy.wait()
    up_copy.wait()


def hidden_kernel(y_ref, out_ref, plain_ref, ordered_ref):
    f32 = jnp.float32
    bf16 = jnp.bfloat16
    rows, width = plain_ref.shape
    share = CAPACITY // TP
    sources = rows // CAPACITY
    back = f32(1.0 / ROW_SCALE)
    peak = jnp.zeros((8, width), f32)
    step = share * sources
    for i in range(TP):
        gate = y_ref[i * step : (i + 1) * step, :width] * back
        up = y_ref[i * step : (i + 1) * step, width:] * back
        hidden = (gate / (1.0 + jnp.exp(-gate)) * up).astype(bf16).astype(f32)
        plain_ref[i * step : (i + 1) * step, :] = hidden
        peak = jnp.maximum(peak, jnp.max(jnp.abs(hidden).reshape(step // 8, 8, width), axis=0))
    top = jnp.max(jnp.max(peak, axis=1, keepdims=True), axis=0, keepdims=True)
    index = jnp.zeros((1, 1), f32)
    scale = jnp.full((1, 1), 2.0**71, f32)
    for i in range(1, LEVELS):
        reached = top >= f32(2.0 ** (8 * i - 64))
        index = jnp.where(reached, f32(i), index)
        scale = jnp.where(reached, f32(2.0 ** (71 - 8 * i)), scale)
    for i in range(TP):
        for j in range(share):
            part = plain_ref[pl.ds(i * step + j, sources, stride=share), :]
            ordered_ref[pl.ds(i * share + j, sources, stride=CAPACITY), :] = part
    out_ref[:rows, :] = (ordered_ref[...] * scale).astype(bf16)
    out_ref[rows:, :] = jnp.broadcast_to(index, (16, width)).astype(bf16)


def combine_kernel(hot_ref, column_ref, rows_ref, out_ref):
    picks, tokens, slots = hot_ref.shape
    hot = hot_ref[...].reshape(picks * tokens, slots)
    picked = jnp.dot(hot, rows_ref[...], preferred_element_type=jnp.float32)
    total = column_ref[0] * picked[:tokens]
    for k in range(1, picks):
        total = total + column_ref[k] * picked[k * tokens : (k + 1) * tokens]
    out_ref[...] = total.astype(jnp.bfloat16)


def route_experts(
    moe_rows, norm_gain, group_choice, member_choice, route_weight, w_gate, w_up, w_down, last_rows
):
    bf16 = jnp.bfloat16
    tokens, width = moe_rows.shape
    share = CAPACITY // TP
    slots = EXPERTS * share
    mine = lax.axis_index("tp").astype(jnp.int32).reshape(1)
    whole = pl.BlockSpec(memory_space=pltpu.VMEM)
    scalar = pl.BlockSpec(memory_space=pltpu.SMEM)
    outside = pl.BlockSpec(memory_space=pl.ANY)
    outgoing, places = pl.pallas_call(
        dispatch_kernel,
        in_specs=[scalar, outside, outside, outside, outside],
        out_specs=[outside, whole],
        out_shape=[
            jax.ShapeDtypeStruct((EXPERTS, share * width // LANES, LANES), bf16),
            pltpu.VMEM((TOP, tokens), jnp.int32),
        ],
        scratch_shapes=[
            pltpu.VMEM((1, tokens), jnp.int32),
            pltpu.VMEM((TOP, tokens), jnp.int32),
            pltpu.VMEM((tokens, width), bf16),
            pltpu.VMEM((1, width), jnp.float32),
            pltpu.VMEM((slots * width // LANES, LANES), jnp.float32),
            pltpu.VMEM((EXPERTS, share * width // LANES, LANES), bf16),
            pltpu.SemaphoreType.DMA((6,)),
        ],
        name="dispatch",
    )(mine, group_choice[None, :], member_choice.T, moe_rows, norm_gain[None, :])
    incoming = lax.all_to_all(outgoing, "ep", 0, 0, tiled=True)
    hots, columns, both = pl.pallas_call(
        prepare_kernel,
        in_specs=[whole, whole, outside, outside],
        out_specs=[whole, whole, whole],
        out_shape=[
            pltpu.VMEM((TOP, tokens, EXPERTS * CAPACITY), bf16),
            pltpu.VMEM((TOP, tokens, LANES), jnp.float32),
            pltpu.VMEM((width, 2 * w_gate.shape[2]), bf16),
        ],
        scratch_shapes=[pltpu.SemaphoreType.DMA, pltpu.SemaphoreType.DMA],
        name="prepare",
    )(near(places), route_weight.T, w_gate[0], w_up[0])
    incoming, last_rows, hots, columns, both = lax.optimization_barrier(
        (incoming, last_rows, hots, columns, both)
    )
    shared = incoming.reshape(slots, width).astype(jnp.float16)
    block_rows = lax.all_gather(shared, "tp", axis=0, tiled=True).astype(bf16)
    total = block_rows.shape[0]
    y = jnp.dot(block_rows, both, preferred_element_type=jnp.float32)
    units = w_gate.shape[2]
    hidden = pl.pallas_call(
        hidden_kernel,
        in_specs=[whole],
        out_specs=whole,
        out_shape=pltpu.VMEM((total + 16, units), bf16),
        scratch_shapes=[pltpu.VMEM((total, units), jnp.float32)] * 2,
        name="hidden",
    )(near(y))
    spread = lax.all_gather(hidden.astype(jnp.float16), "tp", axis=0, tiled=False)
    index = spread[:, total, 0].astype(jnp.float32)
    factor = jnp.full(index.shape, 2.0**-71, jnp.float32)
    for i in range(1, LEVELS):
        factor = jnp.where(index == i, 2.0 ** (8 * i - 71), factor)
    out_width = w_down.shape[2]
    weight = w_down[0].reshape(TP, units, out_width).astype(jnp.float32) * factor[:, None, None]
    produced = jnp.einsum(
        "trk,tko->ro",
        spread[:, :total].astype(bf16),
        weight.astype(bf16),
        preferred_element_type=jnp.float32,
    ).astype(bf16)
    returned = lax.all_to_all(
        produced.reshape(total // CAPACITY, CAPACITY, out_width), "ep", 0, 0, tiled=True
    )
    mixed = pl.pallas_call(
        combine_kernel,
        in_specs=[whole, whole, whole],
        out_specs=whole,
        out_shape=jax.ShapeDtypeStruct((tokens, out_width), bf16),
        name="combine",
    )(near(hots), near(columns), near(returned.reshape(EXPERTS * CAPACITY, out_width)))
    return mixed, last_rows, produced


def shards(
    queries,
    keys_values,
    sink_logits,
    moe_rows,
    norm_gain,
    group_choice,
    member_choice,
    route_weight,
    w_gate,
    w_up,
    w_down,
):
    last_rows = keys_values[:, keys_values.shape[1] - WINDOW :, :]
    mixed, last_rows, produced = route_experts(
        moe_rows,
        norm_gain,
        group_choice,
        member_choice,
        route_weight,
        w_gate,
        w_up,
        w_down,
        last_rows,
    )
    last_rows, sink_logits, produced = lax.optimization_barrier((last_rows, sink_logits, produced))
    edge = passed_along(last_rows)
    attended = attend_window(queries, keys_values, sink_logits, edge)
    return (attended, mixed)


def solution(mesh):
    in_specs = (
        P(("ep", "tp"), None),
        P(None, ("ep", "tp"), None),
        P(),
        P("ep", None),
        P(),
        P("ep"),
        P("ep", None),
        P("ep", None),
        P("ep", None, "tp"),
        P("ep", None, "tp"),
        P("ep", None, "tp"),
    )
    out_specs = (P(("ep", "tp"), None), P("ep", "tp"))
    return jax.shard_map(shards, mesh=mesh, in_specs=in_specs, out_specs=out_specs, check_vma=False)
```
